32 devices in a mesh: sp: 8 (over z, y), tp: 4 (over x, core).
Axes of the slice: x: 2, y: 2, z: 4, core: 2. Of those that a mesh axis runs over, the one named last changes fastest.
Arguments:
- stream_in: bfloat16 [6144, 2048], P(('sp', 'tp')), may hold values from -6 to 6
- query_wide: bfloat16 [6144, 512], P('sp', 'tp'), may hold values from -6 to 6
- key_wide: bfloat16 [6144, 512], P('sp', 'tp'), may hold values from -6 to 6
- value_wide: bfloat16 [6144, 512], P('sp', 'tp'), may hold values from -6 to 6
- gate_wide: bfloat16 [6144, 512], P('sp', 'tp'), may hold values from -6 to 6
- decay_wide: float32 [4, 6144], P('tp', 'sp'), may hold values from -2.3 to 0, as said below
- query_narrow: bfloat16 [6144, 512], P('sp', 'tp'), may hold values from -6 to 6
- key_narrow: bfloat16 [6144, 512], P('sp', 'tp'), may hold values from -6 to 6
- value_narrow: bfloat16 [6144, 512], P('sp', 'tp'), may hold values from -6 to 6
- gate_narrow: bfloat16 [6144, 512], P('sp', 'tp'), may hold values from -6 to 6
- decay_narrow: float32 [8, 6144], P('tp', 'sp'), may hold values from -2.3 to 0, as said below
- output_wide: bfloat16 [512, 2048], P('tp'), may hold values from -0.25 to 0.25
- output_narrow: bfloat16 [512, 2048], P('tp'), may hold values from -0.25 to 0.25
- norm_gain: bfloat16 [2048], replicated, may hold values from 0.099609375 to 1.8984375
- up_weight: bfloat16 [2048, 8192], P('sp', 'tp'), may hold values from -0.125 to 0.125
- down_weight: bfloat16 [8192, 2048], P('tp', 'sp'), may hold values from -0.0625 to 0.0625
Outputs:
- layer_out: bfloat16 [6144, 2048], P(('sp', 'tp'))
The draws below stay inside these ranges and needn't reach their ends.
Inputs may be any that keep to these rules, and one draw needn't show every extreme that they name: `decay_wide`: each entry is the logarithm of one head's retention factor at one position. `decay_narrow`: each entry is the logarithm of one head's retention factor at one position.
All inputs are finite; a program needn't handle non-finite values.
Results may differ from the reference program's by a relative error of at most 0.02.
Values may be sent and summed in bfloat16 or wider, within the bound.
No kernel may reach another device: no remote copies, remote signals or barrier semaphores. Data moves between devices by JAX's collectives and lax.ppermute only.
A program may use at most 128 MiB of HBM per device.

```python
import math
import jax
import jax.numpy as jnp
from jax import lax

D = 2048
FF = 8192
HEADS_W = 4
HEADS_N = 8
HDW = 128
HDN = 64
BLOCK = 128
TOK_DEV = 768
RW = 512
RN = 512
TOKEN_POSITIONS = 6144


spike_count = 3


def log_decay_table(key, count_of_heads, slow_share):
    random_subkey_list = jax.random.split(key, 6)
    slow_heads = jax.random.uniform(random_subkey_list[0], (count_of_heads,), jnp.float32) < slow_share
    slow_rate = jax.random.uniform(random_subkey_list[1], (count_of_heads,), jnp.float32, 0.15, 0.4) * math.log(10.0) / TOKEN_POSITIONS
    fast_rate = 1.0 / jax.random.uniform(random_subkey_list[2], (count_of_heads,), jnp.float32, 30.0, 100.0)
    decay_rate = jnp.where(slow_heads, slow_rate, fast_rate)
    stretch = jnp.exp(jax.random.uniform(random_subkey_list[3], (TOKEN_POSITIONS // TOK_DEV,), jnp.float32, -math.log(2.0), math.log(2.0)))
    stretch = jnp.repeat(stretch, TOK_DEV)
    logarithm_base = -decay_rate[:, None] * stretch[None, :]
    spike_locations = jax.random.randint(random_subkey_list[4], (spike_count,), 0, TOKEN_POSITIONS)
    spike_labels = (jnp.arange(TOKEN_POSITIONS)[None, :] == spike_locations[:, None]).astype(jnp.float32)
    spike_removals = jax.random.uniform(random_subkey_list[5], (count_of_heads, spike_count), jnp.float32, math.log(0.5), math.log(0.8))
    return logarithm_base + jnp.dot(spike_removals, spike_labels)


def draw_decay_wide(key, part):
    share = 0.5
    return log_decay_table(jax.random.fold_in(key, 11), HEADS_W, share)


def draw_decay_narrow(key, part):
    share = 0.5
    return log_decay_table(jax.random.fold_in(key, 23), HEADS_N, share)


def steps_of(own_key, extent, shards, least, largest):
    def one(position, blocks):
        draws = jax.random.uniform(jax.random.fold_in(jax.random.fold_in(own_key, 6), position), (blocks,), jnp.float32, least / len(shards), largest / len(shards))
        return jnp.repeat(jnp.exp(draws), extent[position] // blocks).reshape((-1,) + (1,) * (len(extent) - position - 1))

    level = one(*shards[0])
    for cut in shards[1:]:
        level = level * one(*cut)
    return level


def scatter_about(key, extent, scale, most, pieces=(), kind=jnp.bfloat16):
    loudness = steps_of(key, extent, pieces, -0.22, 0.18) if pieces else 1.0
    drawn = jax.random.normal(key, extent, jnp.float32) * scale * loudness
    return jnp.minimum(jnp.maximum(drawn, -most), most).astype(kind)


def setup_inputs(seed: int = 0) -> dict:
    splits = jax.random.split(jax.random.key(seed), 17)
    return {
        "stream_in": scatter_about(splits[0], (TOKEN_POSITIONS, D), 1.0, 6.0, ((0, 32),)),
        "query_wide": scatter_about(splits[1], (TOKEN_POSITIONS, RW), 1.0, 6.0, ((0, 8), (1, 4))),
        "key_wide": scatter_about(splits[2], (TOKEN_POSITIONS, RW), 1.0, 6.0, ((0, 8), (1, 4))),
        "value_wide": scatter_about(splits[3], (TOKEN_POSITIONS, RW), 1.0, 6.0, ((0, 8), (1, 4))),
        "gate_wide": scatter_about(splits[4], (TOKEN_POSITIONS, RW), 1.0, 6.0, ((0, 8), (1, 4))),
        "decay_wide": draw_decay_wide(jax.random.fold_in(splits[16], 71), 0),
        "query_narrow": scatter_about(splits[6], (TOKEN_POSITIONS, RN), 1.0, 6.0, ((0, 8), (1, 4))),
        "key_narrow": scatter_about(splits[7], (TOKEN_POSITIONS, RN), 1.0, 6.0, ((0, 8), (1, 4))),
        "value_narrow": scatter_about(splits[8], (TOKEN_POSITIONS, RN), 1.0, 6.0, ((0, 8), (1, 4))),
        "gate_narrow": scatter_about(splits[9], (TOKEN_POSITIONS, RN), 1.0, 6.0, ((0, 8), (1, 4))),
        "decay_narrow": draw_decay_narrow(jax.random.fold_in(splits[16], 71), 0),
        "output_wide": scatter_about(splits[11], (RW, D), RW ** -0.5, 0.25, ((0, 4),)),
        "output_narrow": scatter_about(splits[12], (RN, D), RN ** -0.5, 0.25, ((0, 4),)),
        "norm_gain": jnp.clip(1.0 + 0.18 * jax.random.normal(splits[13], (D,), jnp.float32), 0.099609375, 1.8984375).astype(jnp.bfloat16),
        "up_weight": scatter_about(splits[14], (D, FF), D ** -0.5, 0.125, ((0, 8), (1, 4))),
        "down_weight": scatter_about(splits[15], (FF, D), FF ** -0.5, 0.0625, ((0, 4), (1, 8))),
    }


head_eps = 1e-05
norm_eps = 1e-06
rope_base = 10000.0

def rotate(values, places):
    half = values.shape[-1] // 2
    inverse = rope_base ** (-jnp.arange(half, dtype=jnp.float32) / half)
    angles = places[:, None] * inverse[None, :]
    cosine = jnp.cos(angles)[:, None, :]
    sine = jnp.sin(angles)[:, None, :]
    front = values[..., :half]
    back = values[..., half:]
    return jnp.concatenate([front * cosine - back * sine, back * cosine + front * sine], axis=-1)

def block_step(carried, inputs):
    query, keys, values, log_rate = inputs
    running = jnp.cumsum(log_rate, axis=0)
    spread = running[:, None, :] - running[None, :, :]
    length = log_rate.shape[0]
    lower = (jnp.arange(length)[:, None] >= jnp.arange(length)[None, :])[:, :, None]
    factor = jnp.where(lower, jnp.exp(jnp.minimum(spread, 0.0)), 0.0)
    scores = jnp.einsum('thd,shd->tsh', query, keys) * factor
    within = jnp.einsum('tsh,she->the', scores, values)
    across = jnp.einsum('thd,hde->the', query, carried) * jnp.exp(running)[:, :, None]
    tail_decay = jnp.exp(running[-1][None, :] - running)
    updated = jnp.exp(running[-1])[:, None, None] * carried + jnp.einsum('shd,she->hde', keys * tail_decay[:, :, None], values)
    return (updated, within + across)

def retain(query, keys, values, log_rate):
    length, count_of_heads, width = query.shape
    blocks = length // BLOCK

    def shaped(array):
        return array.reshape(blocks, BLOCK, count_of_heads, width)
    rates = log_rate.T.reshape(blocks, BLOCK, count_of_heads)
    carried = jnp.zeros((count_of_heads, width, width), jnp.float32)
    final_state, outputs = lax.scan(block_step, carried, (shaped(query), shaped(keys), shaped(values), rates))
    return outputs.reshape(length, count_of_heads, width)

def head_norm(values):
    centre = values - lax.optimization_barrier(jnp.mean(values, axis=-1, keepdims=True))
    spread = lax.optimization_barrier(jnp.mean(centre * centre, axis=-1, keepdims=True))
    return centre * lax.rsqrt(spread + head_eps)

def group(query, keys, values, gate, log_rate, width, places):
    length = query.shape[0]
    count_of_heads = query.shape[1] // width

    def split(array):
        return array.astype(jnp.float32).reshape(length, count_of_heads, width)
    query_rot = rotate(split(query), places)
    keys_rot = rotate(split(keys), places) * width ** (-0.5)
    normed = head_norm(retain(query_rot, keys_rot, split(values), log_rate)).reshape(length, count_of_heads * width)
    return (jax.nn.silu(gate.astype(jnp.float32)) * normed).astype(jnp.bfloat16)

def reference(stream_in, query_wide, key_wide, value_wide, gate_wide, decay_wide, query_narrow, key_narrow, value_narrow, gate_narrow, decay_narrow, output_wide, output_narrow, norm_gain, up_weight, down_weight):
    places = jnp.arange(TOKEN_POSITIONS, dtype=jnp.float32)
    mixed_wide = group(query_wide, key_wide, value_wide, gate_wide, decay_wide, HDW, places)
    mixed_narrow = group(query_narrow, key_narrow, value_narrow, gate_narrow, decay_narrow, HDN, places)
    mixed_sum = jnp.dot(mixed_wide, output_wide, preferred_element_type=jnp.float32) + jnp.dot(mixed_narrow, output_narrow, preferred_element_type=jnp.float32)
    middle = (stream_in.astype(jnp.float32) + mixed_sum).astype(jnp.bfloat16)
    middle_f = middle.astype(jnp.float32)
    normed_rows = (middle_f * lax.rsqrt(lax.optimization_barrier(jnp.mean(middle_f * middle_f, axis=-1, keepdims=True)) + norm_eps) * norm_gain.astype(jnp.float32)).astype(jnp.bfloat16)
    up_sum = jnp.dot(normed_rows, up_weight, preferred_element_type=jnp.float32)
    hidden = jnp.square(jax.nn.relu(up_sum)).astype(jnp.bfloat16)
    down_sum = jnp.dot(hidden, down_weight, preferred_element_type=jnp.float32)
    return (middle_f + down_sum).astype(jnp.bfloat16)
```

```python
import functools

import jax
import jax.numpy as jnp
import numpy as np
from jax import lax
from jax.experimental import pallas as pl
from jax.experimental.pallas import tpu as pltpu
from jax.sharding import PartitionSpec as P

HDW = 128
HDN = 64
SPAN = 128

head_eps = 1e-05
norm_eps = 1e-06
rope_base = 10000.0


F32 = jnp.float32
BF16 = jnp.bfloat16
VM = pl.BlockSpec(memory_space=pltpu.VMEM)


def call(kernel, out_shape, count, flops, nbytes, **kw):
    return pl.pallas_call(
        kernel,
        out_shape=out_shape,
        in_specs=[VM] * count,
        out_specs=jax.tree.map(lambda _: VM, out_shape),
        cost_estimate=pl.CostEstimate(flops=flops, bytes_accessed=nbytes, transcendentals=0),
        **kw,
    )


def lane_rates(width, lanes):
    half = width // 2
    lane = np.arange(lanes) % width
    return rope_base ** (-(lane % half).astype(np.float64) / half), np.where(lane < half, -1.0, 1.0)


def offset_tables(length, width, lanes):
    rates, signs = lane_rates(width, lanes)
    angles = np.arange(length, dtype=np.float64)[:, None] * rates[None, :]
    return (
        jnp.asarray(np.cos(angles), F32),
        jnp.asarray(np.sin(angles) * signs[None, :], F32),
    )


def start_rows(start, blocks, lanes):
    starts = (start + SPAN * jnp.arange(blocks, dtype=jnp.int32)).astype(F32)[:, None]
    rows = []
    for width in (HDW, HDN):
        rates, signs = lane_rates(width, lanes)
        angle = starts * jnp.asarray(rates, F32)[None, :]
        rows += [jnp.cos(angle), jnp.sin(angle) * jnp.asarray(signs, F32)[None, :]]
    return jnp.stack(rows)


def lane_iota(shape):
    return lax.broadcasted_iota(jnp.int32, shape, 1)


def rotary(x, cos_at, sin_at, width):
    half = width // 2
    lanes = x.shape[1]
    if lanes == width:
        other = pltpu.roll(x, half, 1)
    else:
        other = jnp.where(
            lane_iota(x.shape) % width < half,
            pltpu.roll(x, lanes - half, 1),
            pltpu.roll(x, half, 1),
        )
    return x * cos_at + other * sin_at


def full_tables(cos_r, sin_r, rows, at):
    cos_all, sin_all = [], []
    for n in range(rows.shape[1]):
        cos_p, sin_p = rows[at, n : n + 1, :], rows[at + 1, n : n + 1, :]
        cos_all.append(cos_r * cos_p - sin_r * sin_p)
        sin_all.append(sin_r * cos_p + cos_r * sin_p)
    return jnp.concatenate(cos_all, axis=0), jnp.concatenate(sin_all, axis=0)


def by_head(low, high, lanes):
    rows = low.shape[0]
    return jnp.where(lane_iota((rows, lanes)) < HDN, low, high)


def state_kernel(kw, vw, kn, vn, col, rows, cwr, swr, cnr, snr, out):
    length, lanes = kw.shape
    c = col[...]
    last = c[length - 1 : length, :]
    tail = jnp.exp(last - c)
    cos_w, sin_w = full_tables(cwr[...], swr[...], rows[...], 0)
    k = rotary(kw[...].astype(F32), cos_w, sin_w, HDW) * (HDW ** (-0.5)) * tail[:, 0:1]
    wide = lax.dot_general(
        k.astype(BF16), vw[...], (((0,), (0,)), ((), ())), preferred_element_type=F32
    )
    cos_n, sin_n = full_tables(cnr[...], snr[...], rows[...], 2)
    k = rotary(kn[...].astype(F32), cos_n, sin_n, HDN) * (HDN ** (-0.5))
    k = k * by_head(tail[:, 1:2], tail[:, 2:3], lanes)
    both = lax.dot_general(
        k.astype(BF16), vn[...], (((0,), (0,)), ((), ())), preferred_element_type=F32
    )
    narrow = jnp.where(lane_iota((HDN, lanes)) < HDN, both[:HDN], both[HDN:])
    total = jnp.exp(last)
    row_w = jnp.broadcast_to(total[:, 0:1], (8, lanes))
    row_n = jnp.broadcast_to(by_head(total[:, 1:2], total[:, 2:3], lanes), (8, lanes))
    out[0:HDW, :] = wide
    out[HDW : HDW + HDN, :] = narrow
    out[HDW + HDN : HDW + HDN + 8, :] = row_w
    out[HDW + HDN + 8 : HDW + HDN + 16, :] = row_n


def local_kernel(qw, kw, vw, qn, kn, vn, col, row, rows, cwr, swr, cnr, snr, ow, on, qws, qns):
    length, lanes = kw.shape
    size = 256 if length % 256 == 0 else 128
    blocks = length // size
    c = col[...]
    grown = jnp.exp(c)

    def turned(q, k, cos_r, sin_r, at, width):
        cos_at, sin_at = full_tables(cos_r[...], sin_r[...], rows[...], at)
        return (
            rotary(q[...].astype(F32), cos_at, sin_at, width),
            (rotary(k[...].astype(F32), cos_at, sin_at, width) * width ** (-0.5)).astype(BF16),
        )

    def attend(q, k, v, i, head):
        total = None
        for j in range(i + 1):
            scores = lax.dot_general(
                q, k[j * size : (j + 1) * size], (((1,), (1,)), ((), ())), preferred_element_type=F32
            )
            spread = c[i * size : (i + 1) * size, head : head + 1] - row[
                head : head + 1, j * size : (j + 1) * size
            ]
            factor = jnp.exp(jnp.minimum(spread, 0.0))
            if i == j:
                t = lax.broadcasted_iota(jnp.int32, (size, size), 0)
                s = lax.broadcasted_iota(jnp.int32, (size, size), 1)
                factor = jnp.where(t >= s, factor, 0.0)
            part = jnp.dot(
                (scores * factor).astype(BF16),
                v[j * size : (j + 1) * size, :],
                preferred_element_type=F32,
            )
            total = part if total is None else total + part
        return total

    q, k = turned(qw, kw, cwr, swr, 0, HDW)
    qws[...] = (q * grown[:, 0:1]).astype(BF16)
    q = q.astype(BF16)
    for i in range(blocks):
        ow[i * size : (i + 1) * size, :] = attend(q[i * size : (i + 1) * size], k, vw, i, 0)
    q, k = turned(qn, kn, cnr, snr, 2, HDN)
    qns[...] = (q * by_head(grown[:, 1:2], grown[:, 2:3], lanes)).astype(BF16)
    for i in range(blocks):
        part = q[i * size : (i + 1) * size]
        low = lane_iota(part.shape) < HDN
        first = attend(jnp.where(low, part, 0.0).astype(BF16), k, vn, i, 1)
        second = attend(jnp.where(low, 0.0, part).astype(BF16), k, vn, i, 2)
        on[i * size : (i + 1) * size, :] = jnp.where(low, first, second)


def finish_kernel(ow, on, qws, qns, state, gw, gn, out):
    lanes = ow.shape[1]
    wide = ow[...] + jnp.dot(qws[...], state[0:HDW, :], preferred_element_type=F32)
    packed = state[HDW : HDW + HDN, :]
    low = lane_iota(packed.shape) < HDN
    zero = jnp.zeros_like(packed)
    square = jnp.concatenate(
        [jnp.where(low, packed, zero), jnp.where(low, zero, packed)], axis=0
    )
    narrow = on[...] + jnp.dot(qns[...], square, preferred_element_type=F32)

    def gated(normed, gate):
        g = gate[...].astype(F32)
        return (g / (1.0 + jnp.exp(-g)) * normed).astype(BF16)

    centre = wide - jnp.mean(wide, axis=1, keepdims=True)
    spread = jnp.mean(centre * centre, axis=1, keepdims=True)
    out[:, 0:lanes] = gated(centre * lax.rsqrt(spread + head_eps), gw)

    low = lane_iota(narrow.shape) < HDN

    def head_mean(x):
        first = jnp.sum(jnp.where(low, x, 0.0), axis=1, keepdims=True)
        second = jnp.sum(jnp.where(low, 0.0, x), axis=1, keepdims=True)
        return jnp.where(low, first, second) * (1.0 / HDN)

    centre = narrow - head_mean(narrow)
    out[:, lanes : 2 * lanes] = gated(
        centre * lax.rsqrt(head_mean(centre * centre) + head_eps), gn
    )


def up_kernel(at, x, *refs):
    *blocks, out = refs
    depth = blocks[0].shape[0] + blocks[1].shape[0]
    total = None
    for n in range(len(blocks) // 2):
        columns = pl.ds(pl.multiple_of(at[n] * depth, 128), depth)
        weight = jnp.concatenate([blocks[2 * n][...], blocks[2 * n + 1][...]], axis=0)
        part = jnp.dot(x[:, columns], weight, preferred_element_type=F32)
        total = part if total is None else total + part
    total = jnp.maximum(total, 0.0)
    out[...] = (total * total).astype(BF16)


def up_project(at, x, blocks):
    width = blocks[0].shape[1]
    tile = 512 if width % 512 == 0 else width
    return pl.pallas_call(
        up_kernel,
        out_shape=jax.ShapeDtypeStruct((x.shape[0], width), BF16),
        grid_spec=pltpu.PrefetchScalarGridSpec(
            num_scalar_prefetch=1,
            grid=(width // tile,),
            in_specs=[pl.BlockSpec(x.shape, lambda n, a: (0, 0))]
            + [pl.BlockSpec((b.shape[0], tile), lambda n, a: (0, n)) for b in blocks],
            out_specs=pl.BlockSpec((x.shape[0], tile), lambda n, a: (0, n)),
        ),
        cost_estimate=pl.CostEstimate(
            flops=2 * x.shape[0] * x.shape[1] * width,
            bytes_accessed=2 * (x.size + x.shape[1] * width + x.shape[0] * width),
            transcendentals=0,
        ),
    )(at, x, *blocks)


def place_kernel(at, middle, *refs):
    *parts, out = refs
    for n, part in enumerate(parts):
        width = part.shape[1] // 2
        for side in range(2):
            columns = pl.ds(pl.multiple_of(at[2 * n + side] * width, 128), width)
            out[:, columns] = (
                middle[:, columns].astype(F32)
                + part[:, side * width : (side + 1) * width]
            ).astype(BF16)


def exchange(array, axis, size, move):
    pairs = [(i, move(i)) for i in range(size)]
    return lax.ppermute(array, axis, [(i, j) for i, j in pairs if j is not None and 0 <= j < size])


def incoming_state(state, sp, tree):
    place = lax.axis_index("sp")
    late = place % 2 == 1
    rows = HDW + HDN

    def scale(pack):
        return jnp.concatenate(
            [jnp.broadcast_to(pack[rows : rows + 1], (HDW, pack.shape[1])),
             jnp.broadcast_to(pack[rows + 8 : rows + 9], (HDN, pack.shape[1]))], axis=0
        )

    own = state.astype(BF16)
    other = exchange(own, "sp", sp, lambda i: i ^ 1)
    first = jnp.where(late, other, own).astype(F32)
    second = jnp.where(late, own, other).astype(F32)
    pair = jnp.concatenate(
        [first[:rows] * scale(second) + second[:rows], first[rows:] * second[rows:]], axis=0
    ).astype(BF16)
    total = jnp.zeros((rows, state.shape[1]), F32)
    decay = None
    for step in range(1, sp // 2):
        got = exchange(pair, "sp", sp, lambda i: i + 2 * step).astype(F32)
        total = total + (got[:rows] if decay is None else got[:rows] * decay)
        decay = scale(got) if decay is None else decay * scale(got)
    return jnp.where(late, total * scale(first) + first[:rows], total).astype(BF16)


def retention(tensors, sp):
    (qw, kw, vw, gw, dw, qn, kn, vn, gn, dn) = tensors
    length, lanes = qw.shape
    start = lax.axis_index("sp") * length
    rows = start_rows(start, length // SPAN, lanes)
    tables = offset_tables(SPAN, HDW, lanes) + offset_tables(SPAN, HDN, lanes)
    running = jnp.cumsum(jnp.concatenate([dw, dn], axis=0), axis=1)
    running = jnp.pad(running, ((0, 8 - running.shape[0]), (0, 0)))
    col = running.T
    sds = jax.ShapeDtypeStruct
    unit = length * lanes
    state = call(
        state_kernel, sds((HDW + HDN + 16, lanes), F32), 10, 4 * unit * lanes, 24 * unit
    )(kw, vw, kn, vn, col, rows, *tables)
    ow, on, qws, qns = call(
        local_kernel,
        (sds((length, lanes), F32),) * 2 + (sds((length, lanes), BF16),) * 2,
        13,
        8 * unit * length,
        40 * unit,
    )(qw, kw, vw, qn, kn, vn, col, running, rows, *tables)
    incoming = incoming_state(state, sp, None)
    return call(
        finish_kernel, sds((length, 2 * lanes), BF16), 7, 4 * unit * lanes, 24 * unit
    )(ow, on, qws, qns, incoming, gw, gn)


def row_norm(middle, norm_gain):
    middle_f = middle.astype(F32)
    scale = lax.rsqrt(jnp.mean(middle_f * middle_f, axis=-1, keepdims=True) + norm_eps)
    return (middle_f * scale * norm_gain.astype(F32)).astype(BF16)


def to_middle(mixed, stream_in, output_wide, output_narrow, tp):
    mine = lax.axis_index("tp")
    rows = stream_in.shape[0]
    own = jnp.concatenate([output_wide, output_narrow], axis=0)
    weights = [own]
    pieces = [lax.dynamic_slice_in_dim(mixed, mine * rows, rows, 0)]
    for m in range(1, tp):
        low = m & (m - 1)
        weights.append(
            exchange(weights[low], "tp", tp, lambda i: i ^ (m ^ low))
        )
        piece = lax.dynamic_slice_in_dim(mixed, (mine ^ m) * rows, rows, 0)
        pieces.append(exchange(piece, "tp", tp, lambda i: i ^ m))
    mixed_sum = jnp.dot(
        jnp.concatenate(pieces, axis=1),
        jnp.concatenate(weights, axis=0),
        preferred_element_type=F32,
    )
    return (stream_in.astype(F32) + mixed_sum).astype(BF16)


def plane_feed_forward(middle, normed, up_weight, down_weight, sp, tp):
    z, y = lax.axis_index("sp") // 2, lax.axis_index("sp") % 2
    core = lax.axis_index("tp") % 2
    at_end = (z == 0) | (z == 3)
    both = ("sp", "tp")

    def swap_y_core(array):
        def move(i):
            s, t = divmod(i, tp)
            return ((s & ~1) | (t & 1)) * tp + ((t & ~1) | (s & 1))

        return exchange(array, both, sp * tp, move)

    def along_z(array, table):
        return exchange(array, "sp", sp, lambda i: table[i // 2] * 2 + i % 2 if i // 2 in table else None)

    def other_core(array):
        return exchange(array, "tp", tp, lambda i: i ^ 1)

    def gather(block):
        own = swap_y_core(block)
        near = along_z(own, {0: 1, 1: 0, 2: 3, 3: 2})
        cross = along_z(own, {1: 2, 2: 1})
        outward = along_z(cross, {1: 0, 2: 3})
        inward = along_z(near, {1: 2, 2: 1})
        far = jnp.where(at_end, outward, inward)
        last = along_z(far, {1: 0, 2: 3})
        final = jnp.where(at_end, last, cross)
        return [own, near, far, final]

    slots = [z, z ^ 1, (z + 2) % 4, (z ^ 1) ^ 2]

    half = up_weight.shape[0] // 2
    up_low, up_high = gather(up_weight[:half]), gather(up_weight[half:])
    half = down_weight.shape[0] // 2
    down_low, down_high = gather(down_weight[:half]), gather(down_weight[half:])

    rows = normed.shape[0] // 2

    def by_x(array):
        return exchange(array, "tp", tp, lambda i: i ^ 2)

    def by_y(array):
        return exchange(array, "sp", sp, lambda i: i ^ 1)

    first, second = normed[:rows], normed[rows:]
    first = jnp.concatenate([first, by_x(first)], axis=0)
    second = jnp.concatenate([second, by_y(second)], axis=0)
    plane = jnp.concatenate([first, by_y(first), second, by_x(second)], axis=0)

    order, blocks = [], []
    for s in range(4):
        order += [slots[s] * 2 + core, slots[s] * 2 + 1 - core]
        blocks += [up_low[s], up_high[s], other_core(up_low[s]), other_core(up_high[s])]
    order = jnp.stack(order).astype(jnp.int32)
    hidden = up_project(order, plane, blocks)

    sums = []
    for s in range(4):
        low, high = down_low[s], down_high[s]
        weight = jnp.concatenate(
            [
                jnp.concatenate([low, high], axis=0),
                jnp.concatenate([other_core(low), other_core(high)], axis=0),
            ],
            axis=1,
        )
        part = jnp.dot(hidden, weight, preferred_element_type=F32)
        low, high = part[: 4 * rows], part[4 * rows :]
        low = low[: 2 * rows] + by_y(low[2 * rows :].astype(BF16)).astype(F32)
        high = high[: 2 * rows] + by_x(high[2 * rows :].astype(BF16)).astype(F32)
        low = low[:rows] + by_x(low[rows:].astype(BF16)).astype(F32)
        high = high[:rows] + by_y(high[rows:].astype(BF16)).astype(F32)
        sums.append(jnp.concatenate([low, high], axis=0))
    return pl.pallas_call(
        place_kernel,
        out_shape=jax.ShapeDtypeStruct(middle.shape, BF16),
        in_specs=[pl.BlockSpec(memory_space=pltpu.SMEM)] + [VM] * 5,
        out_specs=VM,
        cost_estimate=pl.CostEstimate(flops=middle.size, bytes_accessed=8 * middle.size, transcendentals=0),
    )(order, middle, *sums)


def group_feed_forward(middle, normed):
    def run(up_weight, down_weight):
        rows = lax.all_gather(normed, "tp", axis=0, tiled=True)
        up_sum = jnp.dot(
            rows, lax.all_gather(up_weight, "sp", axis=0, tiled=True), preferred_element_type=F32
        )
        hidden = jnp.square(jax.nn.relu(up_sum)).astype(BF16)
        down_sum = jnp.dot(
            hidden, lax.all_gather(down_weight, "sp", axis=1, tiled=True), preferred_element_type=F32
        )
        down_rows = lax.psum_scatter(
            down_sum.astype(BF16), "tp", scatter_dimension=0, tiled=True
        ).astype(F32)
        return (middle.astype(F32) + down_rows).astype(BF16)

    return run


def on_device(sp, tp, stream_in, *rest):
    *tensors, output_wide, output_narrow, norm_gain, up_weight, down_weight = rest
    mixed = retention(tensors, sp)
    middle = to_middle(mixed, stream_in, output_wide, output_narrow, tp)
    normed = row_norm(middle, norm_gain)
    if sp == 8 and tp == 4:
        return plane_feed_forward(middle, normed, up_weight, down_weight, sp, tp)
    return group_feed_forward(middle, normed)(up_weight, down_weight)


def solution(mesh):
    split = P("sp", "tp")
    in_specs = (
        (P(("sp", "tp"), None),)
        + ((split,) * 4 + (P("tp", "sp"),)) * 2
        + (P("tp", None), P("tp", None), P(), split, P("tp", "sp"))
    )
    body = functools.partial(on_device, mesh.shape["sp"], mesh.shape["tp"])
    return jax.shard_map(
        body, mesh=mesh, in_specs=in_specs, out_specs=P(("sp", "tp"), None), check_vma=False
    )
```

```python
import functools

import jax
import jax.numpy as jnp
import numpy as np
from jax import lax
from jax.experimental import pallas as pl
from jax.experimental.pallas import tpu as pltpu
from jax.sharding import PartitionSpec as P

HDW = 128
HDN = 64
SPAN = 128

head_eps = 1e-05
norm_eps = 1e-06
rope_base = 10000.0


F32 = jnp.float32
BF16 = jnp.bfloat16
VM = pl.BlockSpec(memory_space=pltpu.VMEM)


def call(kernel, out_shape, count, flops, nbytes, **kw):
    return pl.pallas_call(
        kernel,
        out_shape=out_shape,
        in_specs=[VM] * count,
        out_specs=jax.tree.map(lambda _: VM, out_shape),
        cost_estimate=pl.CostEstimate(flops=flops, bytes_accessed=nbytes, transcendentals=0),
        **kw,
    )


def scalar_call(kernel, out_shape, count, flops, nbytes):
    return pl.pallas_call(
        kernel,
        out_shape=out_shape,
        in_specs=[pl.BlockSpec(memory_space=pltpu.SMEM)] + [VM] * count,
        out_specs=VM,
        cost_estimate=pl.CostEstimate(flops=flops, bytes_accessed=nbytes, transcendentals=0),
    )


def lane_rates(width, lanes):
    half = width // 2
    lane = np.arange(lanes) % width
    return rope_base ** (-(lane % half).astype(np.float64) / half), np.where(lane < half, -1.0, 1.0)


def offset_tables(length, width, lanes):
    rates, signs = lane_rates(width, lanes)
    angles = np.arange(length, dtype=np.float64)[:, None] * rates[None, :]
    return (
        jnp.asarray(np.cos(angles), F32),
        jnp.asarray(np.sin(angles) * signs[None, :], F32),
    )


def start_rows(start, blocks, lanes):
    starts = (start + SPAN * jnp.arange(blocks, dtype=jnp.int32)).astype(F32)[:, None]
    rows = []
    for width in (HDW, HDN):
        rates, signs = lane_rates(width, lanes)
        angle = starts * jnp.asarray(rates, F32)[None, :]
        rows += [jnp.cos(angle), jnp.sin(angle) * jnp.asarray(signs, F32)[None, :]]
    return jnp.stack(rows)


def lane_iota(shape):
    return lax.broadcasted_iota(jnp.int32, shape, 1)


def rotary(x, cos_at, sin_at, width):
    half = width // 2
    lanes = x.shape[1]
    if lanes == width:
        other = pltpu.roll(x, half, 1)
    else:
        other = jnp.where(
            lane_iota(x.shape) % width < half,
            pltpu.roll(x, lanes - half, 1),
            pltpu.roll(x, half, 1),
        )
    return x * cos_at + other * sin_at


def full_tables(cos_r, sin_r, rows, at):
    cos_all, sin_all = [], []
    for n in range(rows.shape[1]):
        cos_p, sin_p = rows[at, n : n + 1, :], rows[at + 1, n : n + 1, :]
        cos_all.append(cos_r * cos_p - sin_r * sin_p)
        sin_all.append(sin_r * cos_p + cos_r * sin_p)
    return jnp.concatenate(cos_all, axis=0), jnp.concatenate(sin_all, axis=0)


def by_head(low, high, lanes):
    rows = low.shape[0]
    return jnp.where(lane_iota((rows, lanes)) < HDN, low, high)


def state_kernel(kw, vw, kn, vn, col, rows, cwr, swr, cnr, snr, out):
    length, lanes = kw.shape
    c = col[...]
    last = c[length - 1 : length, :]
    tail = jnp.exp(last - c)
    cos_w, sin_w = full_tables(cwr[...], swr[...], rows[...], 0)
    k = rotary(kw[...].astype(F32), cos_w, sin_w, HDW) * (HDW ** (-0.5)) * tail[:, 0:1]
    wide = lax.dot_general(
        k.astype(BF16), vw[...], (((0,), (0,)), ((), ())), preferred_element_type=F32
    )
    cos_n, sin_n = full_tables(cnr[...], snr[...], rows[...], 2)
    k = rotary(kn[...].astype(F32), cos_n, sin_n, HDN) * (HDN ** (-0.5))
    k = k * by_head(tail[:, 1:2], tail[:, 2:3], lanes)
    both = lax.dot_general(
        k.astype(BF16), vn[...], (((0,), (0,)), ((), ())), preferred_element_type=F32
    )
    narrow = jnp.where(lane_iota((HDN, lanes)) < HDN, both[:HDN], both[HDN:])
    total = jnp.exp(last)
    row_w = jnp.broadcast_to(total[:, 0:1], (8, lanes))
    row_n = jnp.broadcast_to(by_head(total[:, 1:2], total[:, 2:3], lanes), (8, lanes))
    out[...] = jnp.concatenate([wide, narrow, row_w, row_n], axis=0).astype(BF16)


def local_kernel(qw, kw, vw, qn, kn, vn, col, row, rows, cwr, swr, cnr, snr, ow, on, qws, qns):
    length, lanes = kw.shape
    size = 256 if length % 256 == 0 else 128
    blocks = length // size
    c = col[...]
    grown = jnp.exp(c)

    def turned(q, k, cos_r, sin_r, at, width):
        cos_at, sin_at = full_tables(cos_r[...], sin_r[...], rows[...], at)
        return (
            rotary(q[...].astype(F32), cos_at, sin_at, width),
            (rotary(k[...].astype(F32), cos_at, sin_at, width) * width ** (-0.5)).astype(BF16),
        )

    def attend(q, k, v, i, head):
        total = None
        for j in range(i + 1):
            scores = lax.dot_general(
                q, k[j * size : (j + 1) * size], (((1,), (1,)), ((), ())), preferred_element_type=F32
            )
            spread = c[i * size : (i + 1) * size, head : head + 1] - row[
                head : head + 1, j * size : (j + 1) * size
            ]
            factor = jnp.exp(jnp.minimum(spread, 0.0))
            if i == j:
                t = lax.broadcasted_iota(jnp.int32, (size, size), 0)
                s = lax.broadcasted_iota(jnp.int32, (size, size), 1)
                factor = jnp.where(t >= s, factor, 0.0)
            part = jnp.dot(
                (scores * factor).astype(BF16),
                v[j * size : (j + 1) * size, :],
                preferred_element_type=F32,
            )
            total = part if total is None else total + part
        return total

    q, k = turned(qw, kw, cwr, swr, 0, HDW)
    qws[...] = (q * grown[:, 0:1]).astype(BF16)
    q = q.astype(BF16)
    for i in range(blocks):
        ow[i * size : (i + 1) * size, :] = attend(q[i * size : (i + 1) * size], k, vw, i, 0)
    q, k = turned(qn, kn, cnr, snr, 2, HDN)
    qns[...] = (q * by_head(grown[:, 1:2], grown[:, 2:3], lanes)).astype(BF16)
    for i in range(blocks):
        part = q[i * size : (i + 1) * size]
        low = lane_iota(part.shape) < HDN
        first = attend(jnp.where(low, part, 0.0).astype(BF16), k, vn, i, 1)
        second = attend(jnp.where(low, 0.0, part).astype(BF16), k, vn, i, 2)
        on[i * size : (i + 1) * size, :] = jnp.where(low, first, second)


STATE = HDW + HDN


def decays(pack):
    lanes = pack.shape[1]
    return jnp.concatenate(
        [
            jnp.broadcast_to(pack[STATE : STATE + 1], (HDW, lanes)),
            jnp.broadcast_to(pack[STATE + 8 : STATE + 9], (HDN, lanes)),
        ],
        axis=0,
    )


def ordered(late, own, other):
    flag = late[0] == 1
    own, other = own[...].astype(F32), other[...].astype(F32)
    return jnp.where(flag, other, own), jnp.where(flag, own, other)


def pair_kernel(late, own, other, out):
    first, second = ordered(late, own, other)
    out[...] = jnp.concatenate(
        [first[:STATE] * decays(second) + second[:STATE], first[STATE:] * second[STATE:]], axis=0
    ).astype(BF16)


def finish_kernel(late, own, other, ow, on, qws, qns, gw, gn, *refs):
    *earlier, out = refs
    lanes = ow.shape[1]
    state, decay = None, None
    for got in earlier:
        got = got[...].astype(F32)
        state = got[:STATE] if state is None else state + got[:STATE] * decay
        decay = decays(got) if decay is None else decay * decays(got)
    first, _ = ordered(late, own, other)
    state = jnp.where(late[0] == 1, state * decays(first) + first[:STATE], state).astype(BF16)
    wide = ow[...] + jnp.dot(qws[...], state[0:HDW, :], preferred_element_type=F32)
    packed = state[HDW:STATE, :]
    low = lane_iota(packed.shape) < HDN
    zero = jnp.zeros_like(packed)
    square = jnp.concatenate(
        [jnp.where(low, packed, zero), jnp.where(low, zero, packed)], axis=0
    )
    narrow = on[...] + jnp.dot(qns[...], square, preferred_element_type=F32)

    def gated(normed, gate):
        g = gate[...].astype(F32)
        return (g / (1.0 + jnp.exp(-g)) * normed).astype(BF16)

    centre = wide - jnp.mean(wide, axis=1, keepdims=True)
    spread = jnp.mean(centre * centre, axis=1, keepdims=True)
    out[:, 0:lanes] = gated(centre * lax.rsqrt(spread + head_eps), gw)

    low = lane_iota(narrow.shape) < HDN

    def head_mean(x):
        first = jnp.sum(jnp.where(low, x, 0.0), axis=1, keepdims=True)
        second = jnp.sum(jnp.where(low, 0.0, x), axis=1, keepdims=True)
        return jnp.where(low, first, second) * (1.0 / HDN)

    centre = narrow - head_mean(narrow)
    out[:, lanes : 2 * lanes] = gated(
        centre * lax.rsqrt(head_mean(centre * centre) + head_eps), gn
    )


def middle_kernel(stream, gain, wide, narrow, *refs):
    *inputs, middle, normed = refs
    count = (len(inputs) + 1) // 2
    pieces, weights = inputs[:count], inputs[count:]
    lanes = wide.shape[0]
    own = pieces[0][...]
    total = jnp.dot(own[:, :lanes], wide[...], preferred_element_type=F32)
    total = total + jnp.dot(own[:, lanes:], narrow[...], preferred_element_type=F32)
    for piece, weight in zip(pieces[1:], weights):
        total = total + jnp.dot(piece[...], weight[...], preferred_element_type=F32)
    rounded = (stream[...].astype(F32) + total).astype(BF16)
    middle[...] = rounded
    x = rounded.astype(F32)
    scale = lax.rsqrt(jnp.mean(x * x, axis=-1, keepdims=True) + norm_eps)
    normed[...] = (x * scale * gain[...].astype(F32)).astype(BF16)


def up_kernel(at, own, first_x, first_y, second_y, second_x, *refs):
    *blocks, out, x = refs
    rows = first_x.shape[0]

    @pl.when(pl.program_id(0) == 0)
    def _():
        x[0:rows, :] = own[0:rows, :]
        x[rows : 2 * rows, :] = first_x[...]
        x[2 * rows : 4 * rows, :] = first_y[...]
        x[4 * rows : 5 * rows, :] = own[rows : 2 * rows, :]
        x[5 * rows : 6 * rows, :] = second_y[...]
        x[6 * rows : 8 * rows, :] = second_x[...]

    depth = blocks[0].shape[0]
    total = None
    for n, block in enumerate(blocks):
        columns = pl.ds(pl.multiple_of(at[n] * depth, 128), depth)
        part = jnp.dot(x[:, columns], block[...], preferred_element_type=F32)
        total = part if total is None else total + part
    total = jnp.maximum(total, 0.0)
    out[...] = (total * total).astype(BF16)


def up_project(at, pieces, blocks):
    width = blocks[0].shape[1]
    rows, depth = 8 * pieces[1].shape[0], pieces[1].shape[1]
    tile = 512 if width % 512 == 0 else width
    return pl.pallas_call(
        up_kernel,
        out_shape=jax.ShapeDtypeStruct((rows, width), BF16),
        grid_spec=pltpu.PrefetchScalarGridSpec(
            num_scalar_prefetch=1,
            grid=(width // tile,),
            in_specs=[pl.BlockSpec(p.shape, lambda n, a: (0, 0)) for p in pieces]
            + [pl.BlockSpec((b.shape[0], tile), lambda n, a: (0, n)) for b in blocks],
            out_specs=pl.BlockSpec((rows, tile), lambda n, a: (0, n)),
            scratch_shapes=[pltpu.VMEM((rows, depth), BF16)],
        ),
        cost_estimate=pl.CostEstimate(
            flops=2 * rows * depth * width,
            bytes_accessed=2 * (rows * depth + depth * width + rows * width),
            transcendentals=0,
        ),
    )(at, *pieces, *blocks)


def down_kernel(hidden, *refs):
    *blocks, keep_first, send_first, keep_second, send_second = refs
    half = hidden.shape[0] // 2
    quarter = half // 2
    for n, block in enumerate(blocks):
        width = block.shape[1]
        columns = slice(n * width, (n + 1) * width)
        part = jnp.dot(hidden[0:half, :], block[...], preferred_element_type=F32)
        keep_first[:, columns] = part[:quarter]
        send_first[:, columns] = part[quarter:].astype(BF16)
        part = jnp.dot(hidden[half:, :], block[...], preferred_element_type=F32)
        keep_second[:, columns] = part[:quarter]
        send_second[:, columns] = part[quarter:].astype(BF16)


def down_project(hidden, blocks):
    rows, depth = hidden.shape
    width = sum(b.shape[1] for b in blocks)
    sds = jax.ShapeDtypeStruct
    shape = (rows // 4, width)
    return call(
        down_kernel,
        (sds(shape, F32), sds(shape, BF16)) * 2,
        1 + len(blocks),
        2 * rows * depth * width,
        2 * (rows * depth + depth * width + 2 * rows * width),
    )(hidden, *blocks)


def fold_kernel(keep, got, stay, send):
    total = keep[...] + got[...].astype(F32)
    half = total.shape[0] // 2
    stay[...] = total[:half]
    send[...] = total[half:].astype(BF16)


def fold(keep, got):
    shape = (keep.shape[0] // 2, keep.shape[1])
    sds = jax.ShapeDtypeStruct
    return call(fold_kernel, (sds(shape, F32), sds(shape, BF16)), 2, keep.size, 10 * keep.size)(
        keep, got
    )


def place_kernel(at, middle, *refs):
    *parts, out = refs
    rows = middle.shape[0] // 2
    place = 0
    for n in range(0, len(parts), 4):
        group = parts[n : n + 4]
        for side in range(group[0].shape[1] // 256):
            here = slice(side * 256, (side + 1) * 256)
            columns = pl.ds(pl.multiple_of(at[place] * 256, 128), 256)
            place += 1
            for half in range(2):
                keep, got = group[2 * half], group[2 * half + 1]
                out[half * rows : (half + 1) * rows, columns] = (
                    middle[half * rows : (half + 1) * rows, columns].astype(F32)
                    + keep[:, here]
                    + got[:, here].astype(F32)
                ).astype(BF16)


def exchange(array, axis, size, move):
    pairs = [(i, move(i)) for i in range(size)]
    return lax.ppermute(array, axis, [(i, j) for i, j in pairs if j is not None and 0 <= j < size])


def retention(tensors, sp):
    (qw, kw, vw, gw, dw, qn, kn, vn, gn, dn) = tensors
    length, lanes = qw.shape
    start = lax.axis_index("sp") * length
    rows = start_rows(start, length // SPAN, lanes)
    tables = offset_tables(SPAN, HDW, lanes) + offset_tables(SPAN, HDN, lanes)
    running = jnp.cumsum(jnp.concatenate([dw, dn], axis=0), axis=1)
    running = jnp.pad(running, ((0, 8 - running.shape[0]), (0, 0)))
    col = running.T
    sds = jax.ShapeDtypeStruct
    unit = length * lanes
    state = call(
        state_kernel, sds((HDW + HDN + 16, lanes), BF16), 10, 4 * unit * lanes, 24 * unit
    )(kw, vw, kn, vn, col, rows, *tables)
    ow, on, qws, qns = call(
        local_kernel,
        (sds((length, lanes), F32),) * 2 + (sds((length, lanes), BF16),) * 2,
        13,
        8 * unit * length,
        40 * unit,
    )(qw, kw, vw, qn, kn, vn, col, running, rows, *tables)
    late = (lax.axis_index("sp") % 2).astype(jnp.int32)[None]
    other = exchange(state, "sp", sp, lambda i: i ^ 1)
    pair = scalar_call(pair_kernel, sds(state.shape, BF16), 2, unit, 6 * state.size)(
        late, state, other
    )
    earlier = [exchange(pair, "sp", sp, lambda i: i + 2 * n) for n in range(1, sp // 2)]
    return scalar_call(
        finish_kernel, sds((length, 2 * lanes), BF16), 8 + len(earlier), 4 * unit * lanes, 24 * unit
    )(late, state, other, ow, on, qws, qns, gw, gn, *earlier), other


def to_middle(mixed, stream_in, output_wide, output_narrow, norm_gain, tp):
    mine = lax.axis_index("tp")
    rows = stream_in.shape[0]
    weights = [jnp.concatenate([output_wide, output_narrow], axis=0)]
    pieces = [lax.dynamic_slice_in_dim(mixed, mine * rows, rows, 0)]
    for m in range(1, tp):
        low = m & (m - 1)
        weights.append(exchange(weights[low], "tp", tp, lambda i: i ^ (m ^ low)))
        piece = lax.dynamic_slice_in_dim(mixed, (mine ^ m) * rows, rows, 0)
        pieces.append(exchange(piece, "tp", tp, lambda i: i ^ m))
    sds = jax.ShapeDtypeStruct(stream_in.shape, BF16)
    return call(
        middle_kernel,
        (sds, sds),
        3 + 2 * tp,
        2 * rows * mixed.shape[1] * tp * stream_in.shape[1],
        8 * stream_in.size,
    )(stream_in, norm_gain[None, :], output_wide, output_narrow, *pieces, *weights[1:])


def tie(array, *after):
    return lax.optimization_barrier((array, *after))[0]


def plane_layer(tensors, stream_in, output_wide, output_narrow, norm_gain, up_weight, down_weight, sp, tp):
    z, y = lax.axis_index("sp") // 2, lax.axis_index("sp") % 2
    core = lax.axis_index("tp") % 2
    at_end = (z == 0) | (z == 3)

    def swap_y_core(array, after=()):
        def move(i):
            s, t = divmod(i, tp)
            return None if s & 1 == t & 1 else (s ^ 1) * tp + (t ^ 1)

        got = exchange(tie(array, *after), ("sp", "tp"), sp * tp, move)
        return jnp.where(y == core, array, got)

    def along_z(array, table):
        return exchange(array, "sp", sp, lambda i: table[i // 2] * 2 + i % 2 if i // 2 in table else None)

    def ends(array):
        return along_z(array, {0: 1, 1: 0, 2: 3, 3: 2})

    def middles(array):
        return along_z(array, {1: 2, 2: 1})

    def outwards(array):
        return along_z(array, {1: 0, 2: 3})

    def by_x(array):
        return exchange(array, "tp", tp, lambda i: i ^ 2)

    def by_y(array):
        return exchange(array, "sp", sp, lambda i: i ^ 1)

    def both_cores(slot):
        return [slot, exchange(slot, "tp", tp, lambda i: i ^ 1)]

    slots = [z, z ^ 1, (z + 2) % 4, (z ^ 1) ^ 2]
    order = jnp.stack([s * 2 + c for s in slots for c in (core, 1 - core)]).astype(jnp.int32)

    up_own = swap_y_core(up_weight)
    up_near, up_cross = ends(up_own), middles(up_own)

    mixed, other_state = retention(tensors, sp)

    down_own = swap_y_core(down_weight, (other_state,))
    down_near = ends(down_own)
    up_in = middles(up_near)
    up_out = outwards(up_cross)
    down_cross = middles(tie(down_own, up_near))
    up_last = outwards(up_in)

    middle, normed = to_middle(mixed, stream_in, output_wide, output_narrow, norm_gain, tp)

    rows = normed.shape[0] // 2
    first, second = normed[:rows], normed[rows:]
    first_x, second_y = by_x(first), by_y(second)
    first_y = by_y(jnp.concatenate([first, first_x], axis=0))
    second_x = by_x(jnp.concatenate([second, second_y], axis=0))
    there = (first_y, second_x)

    down_out = outwards(tie(down_cross, *there))
    down_in = middles(tie(down_near, *there))
    up_far = jnp.where(at_end, tie(up_out, *there), up_in)
    up_final = jnp.where(at_end, up_last, up_cross)
    down_last = outwards(tie(down_in, up_final))

    hidden = up_project(
        order,
        [normed, first_x, first_y, second_y, second_x],
        sum([both_cores(u) for u in (up_own, up_near, up_far, up_final)], []),
    )

    sums = []

    def down(group):
        blocks = sum([both_cores(d) for d in group], [])
        keep_first, send_first, keep_second, send_second = down_project(hidden, blocks)
        keep_first, send_first = fold(keep_first, by_y(send_first))
        keep_second, send_second = fold(keep_second, by_x(send_second))
        sums.extend([keep_first, by_x(send_first), keep_second, by_y(send_second)])
        return keep_first, keep_second

    after = down([down_own, down_near])
    down_far = jnp.where(at_end, tie(down_out, hidden), down_in)
    after = down([down_far])
    down_final = jnp.where(at_end, tie(down_last, *after), down_cross)
    down([down_final])
    return scalar_call(
        place_kernel,
        jax.ShapeDtypeStruct(middle.shape, BF16),
        1 + len(sums),
        middle.size,
        8 * middle.size,
    )(order, middle, *sums)


def group_feed_forward(middle, normed):
    def run(up_weight, down_weight):
        rows = lax.all_gather(normed, "tp", axis=0, tiled=True)
        up_sum = jnp.dot(
            rows, lax.all_gather(up_weight, "sp", axis=0, tiled=True), preferred_element_type=F32
        )
        hidden = jnp.square(jax.nn.relu(up_sum)).astype(BF16)
        down_sum = jnp.dot(
            hidden, lax.all_gather(down_weight, "sp", axis=1, tiled=True), preferred_element_type=F32
        )
        down_rows = lax.psum_scatter(
            down_sum.astype(BF16), "tp", scatter_dimension=0, tiled=True
        ).astype(F32)
        return (middle.astype(F32) + down_rows).astype(BF16)

    return run


def on_device(sp, tp, stream_in, *rest):
    *tensors, output_wide, output_narrow, norm_gain, up_weight, down_weight = rest
    if sp == 8 and tp == 4:
        return plane_layer(
            tensors, stream_in, output_wide, output_narrow, norm_gain, up_weight, down_weight, sp, tp
        )
    mixed, _ = retention(tensors, sp)
    middle, normed = to_middle(mixed, stream_in, output_wide, output_narrow, norm_gain, tp)
    return group_feed_forward(middle, normed)(up_weight, down_weight)


def solution(mesh):
    split = P("sp", "tp")
    in_specs = (
        (P(("sp", "tp"), None),)
        + ((split,) * 4 + (P("tp", "sp"),)) * 2
        + (P("tp", None), P("tp", None), P(), split, P("tp", "sp"))
    )
    body = functools.partial(on_device, mesh.shape["sp"], mesh.shape["tp"])
    return jax.shard_map(
        body, mesh=mesh, in_specs=in_specs, out_specs=P(("sp", "tp"), None), check_vma=False
    )
```

```python
import functools

import jax
import jax.numpy as jnp
import numpy as np
from jax import lax
from jax.experimental import pallas as pl
from jax.experimental.pallas import tpu as pltpu
from jax.sharding import PartitionSpec as P


HDW = 128
HDN = 64
SPAN = 128

head_eps = 1e-05
norm_eps = 1e-06
rope_base = 10000.0


F32 = jnp.float32
BF16 = jnp.bfloat16
VM = pl.BlockSpec(memory_space=pltpu.VMEM)


def call(kernel, out_shape, count, flops, nbytes):
    return pl.pallas_call(
        kernel,
        out_shape=out_shape,
        in_specs=[VM] * count,
        out_specs=jax.tree.map(lambda _: VM, out_shape),
        cost_estimate=pl.CostEstimate(flops=flops, bytes_accessed=nbytes, transcendentals=0),
    )


def scalar_call(kernel, out_shape, count, flops, nbytes, scratch=()):
    return pl.pallas_call(
        kernel,
        out_shape=out_shape,
        in_specs=[pl.BlockSpec(memory_space=pltpu.SMEM)] + [VM] * count,
        out_specs=jax.tree.map(lambda _: VM, out_shape),
        scratch_shapes=scratch,
        cost_estimate=pl.CostEstimate(flops=flops, bytes_accessed=nbytes, transcendentals=0),
    )


def lane_rates(width, lanes):
    half = width // 2
    lane = np.arange(lanes) % width
    return rope_base ** (-(lane % half).astype(np.float64) / half), np.where(lane < half, -1.0, 1.0)


def offset_tables(length, width, lanes):
    rates, signs = lane_rates(width, lanes)
    angles = np.arange(length, dtype=np.float64)[:, None] * rates[None, :]
    return (
        jnp.asarray(np.cos(angles), F32),
        jnp.asarray(np.sin(angles) * signs[None, :], F32),
    )


def start_rows(places, length, lanes):
    starts = SPAN * np.arange(places * (length // SPAN), dtype=np.float64)[:, None]
    rows = []
    for width in (HDW, HDN):
        rates, signs = lane_rates(width, lanes)
        angle = starts * rates[None, :]
        rows += [np.cos(angle), np.sin(angle) * signs[None, :]]
    return jnp.asarray(np.stack(rows).reshape(4, places, length // SPAN, lanes), F32)


def lane_iota(shape):
    return lax.broadcasted_iota(jnp.int32, shape, 1)


def rotary(x, cos_at, sin_at, width):
    half = width // 2
    lanes = x.shape[1]
    if lanes == width:
        other = pltpu.roll(x, half, 1)
    else:
        other = jnp.where(
            lane_iota(x.shape) % width < half,
            pltpu.roll(x, lanes - half, 1),
            pltpu.roll(x, half, 1),
        )
    return x * cos_at + other * sin_at


def full_tables(cos_r, sin_r, rows, at):
    cos_all, sin_all = [], []
    for n in range(rows.shape[1]):
        cos_p, sin_p = rows[at, n : n + 1, :], rows[at + 1, n : n + 1, :]
        cos_all.append(cos_r * cos_p - sin_r * sin_p)
        sin_all.append(sin_r * cos_p + cos_r * sin_p)
    return jnp.concatenate(cos_all, axis=0), jnp.concatenate(sin_all, axis=0)


def by_head(low, high, lanes):
    rows = low.shape[0]
    return jnp.where(lane_iota((rows, lanes)) < HDN, low, high)


def state_kernel(kw, vw, kn, vn, dw, dn, rows, cwr, swr, cnr, snr, out, col, row):
    length, lanes = kw.shape
    head = lax.broadcasted_iota(jnp.int32, (8, length), 0)
    c = jnp.where(head == 0, dw[0:1, :], 0.0)
    for n in range(dn.shape[0]):
        c = jnp.where(head == n + 1, dn[n : n + 1, :], c)
    step = 1
    while step < length:
        c = c + jnp.where(lane_iota(c.shape) >= step, pltpu.roll(c, step, 1), 0.0)
        step *= 2
    row[...] = c
    c = c.T
    col[...] = c
    last = c[length - 1 : length, :]
    tail = jnp.exp(last - c)
    cos_w, sin_w = full_tables(cwr[...], swr[...], rows[...], 0)
    k = rotary(kw[...].astype(F32), cos_w, sin_w, HDW) * (HDW ** (-0.5)) * tail[:, 0:1]
    wide = lax.dot_general(
        k.astype(BF16), vw[...], (((0,), (0,)), ((), ())), preferred_element_type=F32
    )
    cos_n, sin_n = full_tables(cnr[...], snr[...], rows[...], 2)
    k = rotary(kn[...].astype(F32), cos_n, sin_n, HDN) * (HDN ** (-0.5))
    k = k * by_head(tail[:, 1:2], tail[:, 2:3], lanes)
    both = lax.dot_general(
        k.astype(BF16), vn[...], (((0,), (0,)), ((), ())), preferred_element_type=F32
    )
    narrow = jnp.where(lane_iota((HDN, lanes)) < HDN, both[:HDN], both[HDN:])
    total = jnp.exp(last)
    row_w = jnp.broadcast_to(total[:, 0:1], (8, lanes))
    row_n = jnp.broadcast_to(by_head(total[:, 1:2], total[:, 2:3], lanes), (8, lanes))
    out[...] = jnp.concatenate([wide, narrow, row_w, row_n], axis=0).astype(BF16)


def local_kernel(qw, kw, vw, qn, kn, vn, col, row, rows, cwr, swr, cnr, snr, ow, on, qws, qns):
    length, lanes = kw.shape
    size = 256 if length % 256 == 0 else 128
    blocks = length // size
    c = col[...]
    grown = jnp.exp(c)

    def turned(q, k, cos_r, sin_r, at, width):
        cos_at, sin_at = full_tables(cos_r[...], sin_r[...], rows[...], at)
        return (
            rotary(q[...].astype(F32), cos_at, sin_at, width),
            (rotary(k[...].astype(F32), cos_at, sin_at, width) * width ** (-0.5)).astype(BF16),
        )

    def attend(q, k, v, i, head):
        total = None
        for j in range(i + 1):
            scores = lax.dot_general(
                q, k[j * size : (j + 1) * size], (((1,), (1,)), ((), ())), preferred_element_type=F32
            )
            spread = c[i * size : (i + 1) * size, head : head + 1] - row[
                head : head + 1, j * size : (j + 1) * size
            ]
            factor = jnp.exp(jnp.minimum(spread, 0.0))
            if i == j:
                t = lax.broadcasted_iota(jnp.int32, (size, size), 0)
                s = lax.broadcasted_iota(jnp.int32, (size, size), 1)
                factor = jnp.where(t >= s, factor, 0.0)
            part = jnp.dot(
                (scores * factor).astype(BF16),
                v[j * size : (j + 1) * size, :],
                preferred_element_type=F32,
            )
            total = part if total is None else total + part
        return total

    q, k = turned(qw, kw, cwr, swr, 0, HDW)
    qws[...] = (q * grown[:, 0:1]).astype(BF16)
    q = q.astype(BF16)
    for i in range(blocks):
        ow[i * size : (i + 1) * size, :] = attend(q[i * size : (i + 1) * size], k, vw, i, 0)
    q, k = turned(qn, kn, cnr, snr, 2, HDN)
    qns[...] = (q * by_head(grown[:, 1:2], grown[:, 2:3], lanes)).astype(BF16)
    for i in range(blocks):
        part = q[i * size : (i + 1) * size]
        low = lane_iota(part.shape) < HDN
        first = attend(jnp.where(low, part, 0.0).astype(BF16), k, vn, i, 1)
        second = attend(jnp.where(low, 0.0, part).astype(BF16), k, vn, i, 2)
        on[i * size : (i + 1) * size, :] = jnp.where(low, first, second)


STATE = HDW + HDN


def decays(pack):
    lanes = pack.shape[1]
    return jnp.concatenate(
        [
            jnp.broadcast_to(pack[STATE : STATE + 1], (HDW, lanes)),
            jnp.broadcast_to(pack[STATE + 8 : STATE + 9], (HDN, lanes)),
        ],
        axis=0,
    )


def ordered(late, own, other):
    flag = late[0] == 1
    own, other = own[...].astype(F32), other[...].astype(F32)
    return jnp.where(flag, other, own), jnp.where(flag, own, other)


def pair_kernel(late, own, other, out):
    first, second = ordered(late, own, other)
    out[...] = jnp.concatenate(
        [first[:STATE] * decays(second) + second[:STATE], first[STATE:] * second[STATE:]], axis=0
    ).astype(BF16)


def finish_kernel(tp, late, own, other, ow, on, qws, qns, gw, gn, *refs):
    earlier, outs, out = refs[: -tp - 1], refs[-tp - 1 : -1], refs[-1]
    lanes = ow.shape[1]
    state, decay = None, None
    for got in earlier:
        got = got[...].astype(F32)
        state = got[:STATE] if state is None else state + got[:STATE] * decay
        decay = decays(got) if decay is None else decay * decays(got)
    first, _ = ordered(late, own, other)
    state = jnp.where(late[0] == 1, state * decays(first) + first[:STATE], state).astype(BF16)
    wide = ow[...] + jnp.dot(qws[...], state[0:HDW, :], preferred_element_type=F32)
    packed = state[HDW:STATE, :]
    low = lane_iota(packed.shape) < HDN
    zero = jnp.zeros_like(packed)
    square = jnp.concatenate(
        [jnp.where(low, packed, zero), jnp.where(low, zero, packed)], axis=0
    )
    narrow = on[...] + jnp.dot(qns[...], square, preferred_element_type=F32)

    def gated(normed, gate):
        g = gate[...].astype(F32)
        return (g / (1.0 + jnp.exp(-g)) * normed).astype(BF16)

    centre = wide - jnp.mean(wide, axis=1, keepdims=True)
    spread = jnp.mean(centre * centre, axis=1, keepdims=True)
    out[:, 0:lanes] = gated(centre * lax.rsqrt(spread + head_eps), gw)

    low = lane_iota(narrow.shape) < HDN

    def head_mean(x):
        first = jnp.sum(jnp.where(low, x, 0.0), axis=1, keepdims=True)
        second = jnp.sum(jnp.where(low, 0.0, x), axis=1, keepdims=True)
        return jnp.where(low, first, second) * (1.0 / HDN)

    centre = narrow - head_mean(narrow)
    out[:, lanes : 2 * lanes] = gated(
        centre * lax.rsqrt(head_mean(centre * centre) + head_eps), gn
    )
    piece = outs[0].shape[0]
    for m, rows in enumerate(outs):
        start = pl.multiple_of(late[1 + m] * piece, 16)
        rows[...] = out[pl.ds(start, piece), :]


def middle_kernel(stream, gain, wide, narrow, *refs):
    *inputs, middle, first, second = refs
    count = (len(inputs) + 1) // 2
    pieces, weights = inputs[:count], inputs[count:]
    lanes = wide.shape[0]
    own = pieces[0][...]
    total = jnp.dot(own[:, :lanes], wide[...], preferred_element_type=F32)
    total = total + jnp.dot(own[:, lanes:], narrow[...], preferred_element_type=F32)
    for piece, weight in zip(pieces[1:], weights):
        total = total + jnp.dot(piece[...], weight[...], preferred_element_type=F32)
    rounded = (stream[...].astype(F32) + total).astype(BF16)
    middle[...] = rounded
    x = rounded.astype(F32)
    scale = lax.rsqrt(jnp.mean(x * x, axis=-1, keepdims=True) + norm_eps)
    normed = (x * scale * gain[...].astype(F32)).astype(BF16)
    half = normed.shape[0] // 2
    first[...] = normed[:half]
    second[...] = normed[half:]


def up_kernel(at, own_a, own_b, x_a, y_a, y_b, x_b, *refs):
    *blocks, out, x = refs
    depth = blocks[0].shape[0]
    rows = own_a.shape[0]

    @pl.when(pl.program_id(0) == 0)
    def _():
        for n, piece in enumerate(
            (own_a, own_b, x_a, x_b.at[:rows], y_a.at[:rows], y_b, y_a.at[rows:], x_b.at[rows:])
        ):
            x[n * rows : (n + 1) * rows, :] = piece[...]

    total = None
    for n, block in enumerate(blocks):
        columns = pl.ds(pl.multiple_of(at[n] * depth, 128), depth)
        part = jnp.dot(x[:, columns], block[...], preferred_element_type=F32)
        total = part if total is None else total + part
    total = jnp.maximum(total, 0.0)
    out[...] = (total * total).astype(BF16)


def up_project(at, pieces, blocks):
    width = blocks[0].shape[1]
    rows, depth = sum(p.shape[0] for p in pieces), pieces[0].shape[1]
    tile = 512
    run = pl.pallas_call(
        up_kernel,
        out_shape=jax.ShapeDtypeStruct((rows, width), BF16),
        grid_spec=pltpu.PrefetchScalarGridSpec(
            num_scalar_prefetch=1,
            grid=(width // tile,),
            in_specs=[pl.BlockSpec(p.shape, lambda n, a: (0, 0)) for p in pieces]
            + [pl.BlockSpec((b.shape[0], tile), lambda n, a: (0, n)) for b in blocks],
            out_specs=pl.BlockSpec((rows, tile), lambda n, a: (0, n)),
            scratch_shapes=[pltpu.VMEM((rows, depth), BF16)],
        ),
        cost_estimate=pl.CostEstimate(
            flops=2 * rows * depth * width,
            bytes_accessed=2 * (rows * depth + depth * width + rows * width),
            transcendentals=0,
        ),
    )
    return run(at, *pieces, *blocks)


SIDE = 256


def place_kernel(at, middle, *refs):
    *parts, out = refs
    place = 0
    for n in range(0, len(parts), 4):
        group = parts[n : n + 4]
        for side in range(group[0].shape[1] // SIDE):
            here = slice(side * SIDE, (side + 1) * SIDE)
            columns = pl.ds(pl.multiple_of(at[place] * SIDE, 128), SIDE)
            place += 1
            total = middle[:, columns].astype(F32)
            for part in group:
                total = total + part[:, here].astype(F32)
            out[:, columns] = total.astype(BF16)


def last_kernel(at, out_in, middle, *refs):
    *parts, out = refs
    total = middle[...].astype(F32)
    for part in parts:
        total = total + part[...].astype(F32)
    out[...] = total.astype(BF16)


def place_last(at, out, middle, parts):
    rows = middle.shape[0]
    skip = middle.shape[1] // SIDE - parts[0].shape[1] // SIDE

    def column(n, a):
        return (0, a[skip + n])

    run = pl.pallas_call(
        last_kernel,
        out_shape=jax.ShapeDtypeStruct(middle.shape, BF16),
        grid_spec=pltpu.PrefetchScalarGridSpec(
            num_scalar_prefetch=1,
            grid=(parts[0].shape[1] // SIDE,),
            in_specs=[pl.BlockSpec(memory_space=pl.ANY), pl.BlockSpec((rows, SIDE), column)]
            + [pl.BlockSpec((rows, SIDE), lambda n, a: (0, n))] * len(parts),
            out_specs=pl.BlockSpec((rows, SIDE), column),
        ),
        input_output_aliases={1: 0},
        cost_estimate=pl.CostEstimate(
            flops=middle.size, bytes_accessed=4 * middle.size, transcendentals=0
        ),
    )
    return run(at, out, middle, *parts)


def exchange(array, axis, size, move):
    pairs = [(i, move(i)) for i in range(size)]
    return lax.ppermute(array, axis, [(i, j) for i, j in pairs if j is not None and 0 <= j < size])


def retention(tensors, sp, tp):
    (qw, kw, vw, gw, dw, qn, kn, vn, gn, dn) = tensors
    length, lanes = qw.shape
    rows = lax.dynamic_index_in_dim(
        start_rows(sp, length, lanes), lax.axis_index("sp"), 1, keepdims=False
    )
    tables = offset_tables(SPAN, HDW, lanes) + offset_tables(SPAN, HDN, lanes)
    sds = jax.ShapeDtypeStruct
    unit = length * lanes
    state, col, running = call(
        state_kernel,
        (sds((STATE + 16, lanes), BF16), sds((length, 8), F32), sds((8, length), F32)),
        11,
        4 * unit * lanes,
        24 * unit,
    )(kw, vw, kn, vn, dw, dn, rows, *tables)
    ow, on, qws, qns = call(
        local_kernel,
        (sds((length, lanes), F32),) * 2 + (sds((length, lanes), BF16),) * 2,
        13,
        8 * unit * length,
        40 * unit,
    )(qw, kw, vw, qn, kn, vn, col, running, rows, *tables)
    mine = lax.axis_index("tp")
    late = jnp.stack([lax.axis_index("sp") % 2] + [mine ^ m for m in range(tp)]).astype(jnp.int32)
    other = exchange(state, "sp", sp, lambda i: i ^ 1)
    pair = scalar_call(pair_kernel, sds(state.shape, BF16), 2, unit, 6 * state.size)(
        late, state, other
    )
    earlier = [exchange(pair, "sp", sp, lambda i: i + 2 * n) for n in range(1, sp // 2)]
    pieces = scalar_call(
        functools.partial(finish_kernel, tp),
        (sds((length // tp, 2 * lanes), BF16),) * tp,
        8 + len(earlier),
        4 * unit * lanes,
        24 * unit,
        [pltpu.VMEM((length, 2 * lanes), BF16)],
    )(late, state, other, ow, on, qws, qns, gw, gn, *earlier)
    return pieces, other


def to_middle(mixed, stream_in, output_wide, output_narrow, norm_gain, tp):
    weights = [jnp.concatenate([output_wide, output_narrow], axis=0)]
    pieces = [mixed[0]]
    for m in range(1, tp):
        low = m & (m - 1)
        weights.append(exchange(weights[low], "tp", tp, lambda i: i ^ (m ^ low)))
        pieces.append(exchange(mixed[m], "tp", tp, lambda i: i ^ m))
    sds = jax.ShapeDtypeStruct
    rows, depth = stream_in.shape
    return call(
        middle_kernel,
        (sds((rows, depth), BF16),) + (sds((rows // 2, depth), BF16),) * 2,
        3 + 2 * tp,
        2 * rows * mixed[0].shape[1] * tp * depth,
        8 * stream_in.size,
    )(stream_in, norm_gain[None, :], output_wide, output_narrow, *pieces, *weights[1:])


def tie(array, *after):
    return lax.optimization_barrier((array, *after))[0]


def plane_layer(tensors, stream_in, output_wide, output_narrow, norm_gain, up_weight, down_weight, sp, tp):
    z, y = lax.axis_index("sp") // 2, lax.axis_index("sp") % 2
    core = lax.axis_index("tp") % 2
    at_end = (z == 0) | (z == 3)

    def swap_y_core(array, after=()):
        def move(i):
            s, t = divmod(i, tp)
            return None if s & 1 == t & 1 else (s ^ 1) * tp + (t ^ 1)

        return exchange(tie(array, *after), ("sp", "tp"), sp * tp, move)

    def along_z(array, table):
        def move(i):
            return table[i // 2] * 2 + i % 2 if i // 2 in table else None

        return exchange(array, "sp", sp, move)

    def ends(array):
        return along_z(array, {0: 1, 1: 0, 2: 3, 3: 2})

    def middles(array):
        return along_z(array, {1: 2, 2: 1})

    def outwards(array):
        return along_z(array, {1: 0, 2: 3})

    def by_x(array):
        return exchange(array, "tp", tp, lambda i: i ^ 2)

    def by_y(array):
        return exchange(array, "sp", sp, lambda i: i ^ 1)

    def both_cores(slot):
        return [slot, exchange(slot, "tp", tp, lambda i: i ^ 1)]

    slots = [z, z ^ 1, (z + 2) % 4, (z ^ 1) ^ 2]
    order = jnp.stack([s * 2 + c for s in slots for c in (core, 1 - core)]).astype(jnp.int32)

    def own_block(block, after=()):
        return jnp.where(y == core, block, swap_y_core(block, after))

    up_own = own_block(up_weight)
    up_near, up_cross = ends(up_own), middles(up_own)

    mixed, other_state = retention(tensors, sp, tp)

    down_own = own_block(down_weight, (other_state,))
    down_near = ends(down_own)
    up_in = middles(up_near)
    up_out = outwards(up_cross)
    down_cross = middles(tie(down_own, up_near))
    up_last = outwards(up_in)

    middle, first, second = to_middle(mixed, stream_in, output_wide, output_narrow, norm_gain, tp)

    x_a, y_b = by_x(first), by_y(second)
    down_in = middles(tie(down_near, y_b))
    y_a = by_y(jnp.concatenate([first, x_a], axis=0))
    x_b = by_x(jnp.concatenate([second, y_b], axis=0))
    there = (y_a, x_b)

    down_out = outwards(down_cross)
    up_far = jnp.where(at_end, up_out, up_in)
    up_final = jnp.where(at_end, tie(up_last, *there), up_cross)
    down_last = outwards(tie(down_in, up_final))

    blocks = []
    for slot in (up_own, up_near, up_far, up_final):
        blocks += both_cores(slot)
    hidden = up_project(order, [first, second, x_a, y_a, y_b, x_b], blocks)

    def down(group):
        blocks = []
        for d in group:
            blocks += both_cores(d)
        part = jnp.dot(
            hidden, jnp.concatenate(blocks, axis=1), preferred_element_type=F32
        ).astype(BF16)
        rows = part.shape[0] // 4
        keep, to_x, to_y, across = (part[m * rows : (m + 1) * rows] for m in range(4))
        return [
            keep,
            exchange(across, ("sp", "tp"), sp * tp, lambda i: i ^ tp ^ 2),
            by_x(to_x),
            by_y(to_y),
        ]

    sums = down([down_own, down_near])
    down_far = jnp.where(at_end, tie(down_out, hidden), down_in)
    sums += down([down_far])
    out = scalar_call(
        place_kernel,
        jax.ShapeDtypeStruct(middle.shape, BF16),
        1 + len(sums),
        middle.size,
        8 * middle.size,
    )(order, middle, *sums)
    down_final = jnp.where(at_end, tie(down_last, out), down_cross)
    return place_last(order, out, middle, down([down_final]))


def group_feed_forward(middle, normed):
    def run(up_weight, down_weight):
        rows = lax.all_gather(normed, "tp", axis=0, tiled=True)
        up_sum = jnp.dot(
            rows, lax.all_gather(up_weight, "sp", axis=0, tiled=True), preferred_element_type=F32
        )
        hidden = jnp.square(jax.nn.relu(up_sum)).astype(BF16)
        down_sum = jnp.dot(
            hidden, lax.all_gather(down_weight, "sp", axis=1, tiled=True), preferred_element_type=F32
        )
        down_rows = lax.psum_scatter(
            down_sum.astype(BF16), "tp", scatter_dimension=0, tiled=True
        ).astype(F32)
        return (middle.astype(F32) + down_rows).astype(BF16)

    return run


def on_device(sp, tp, stream_in, *rest):
    *tensors, output_wide, output_narrow, norm_gain, up_weight, down_weight = rest
    if sp == 8 and tp == 4:
        return plane_layer(
            tensors, stream_in, output_wide, output_narrow, norm_gain, up_weight, down_weight, sp, tp
        )
    mixed, _ = retention(tensors, sp, tp)
    middle, first, second = to_middle(mixed, stream_in, output_wide, output_narrow, norm_gain, tp)
    normed = jnp.concatenate([first, second], axis=0)
    return group_feed_forward(middle, normed)(up_weight, down_weight)


def solution(mesh):
    split = P("sp", "tp")
    in_specs = (
        (P(("sp", "tp"), None),)
        + ((split,) * 4 + (P("tp", "sp"),)) * 2
        + (P("tp", None), P("tp", None), P(), split, P("tp", "sp"))
    )
    sp, tp = mesh.shape["sp"], mesh.shape["tp"]
    return jax.shard_map(
        functools.partial(on_device, sp, tp),
        mesh=mesh,
        in_specs=in_specs,
        out_specs=P(("sp", "tp"), None),
        check_vma=False,
    )
```

```python
import functools

import jax
import jax.numpy as jnp
import numpy as np
from jax import lax
from jax.experimental import pallas as pl
from jax.experimental.pallas import tpu as pltpu
from jax.sharding import PartitionSpec as P


HDW = 128
HDN = 64
SPAN = 128

head_eps = 1e-05
norm_eps = 1e-06
rope_base = 10000.0


F32 = jnp.float32
BF16 = jnp.bfloat16
VM = pl.BlockSpec(memory_space=pltpu.VMEM)


def call(kernel, out_shape, count, flops, nbytes):
    return pl.pallas_call(
        kernel,
        out_shape=out_shape,
        in_specs=[VM] * count,
        out_specs=jax.tree.map(lambda _: VM, out_shape),
        cost_estimate=pl.CostEstimate(flops=flops, bytes_accessed=nbytes, transcendentals=0),
    )


def scalar_call(kernel, out_shape, count, flops, nbytes, scratch=()):
    return pl.pallas_call(
        kernel,
        out_shape=out_shape,
        in_specs=[pl.BlockSpec(memory_space=pltpu.SMEM)] + [VM] * count,
        out_specs=jax.tree.map(lambda _: VM, out_shape),
        scratch_shapes=scratch,
        cost_estimate=pl.CostEstimate(flops=flops, bytes_accessed=nbytes, transcendentals=0),
    )


def lane_rates(width, lanes):
    half = width // 2
    lane = np.arange(lanes) % width
    return rope_base ** (-(lane % half).astype(np.float64) / half), np.where(lane < half, -1.0, 1.0)


def offset_tables(length, width, lanes):
    rates, signs = lane_rates(width, lanes)
    angles = np.arange(length, dtype=np.float64)[:, None] * rates[None, :]
    return (
        jnp.asarray(np.cos(angles), F32),
        jnp.asarray(np.sin(angles) * signs[None, :], F32),
    )


def start_rows(places, length, lanes):
    starts = SPAN * np.arange(places * (length // SPAN), dtype=np.float64)[:, None]
    rows = []
    for width in (HDW, HDN):
        rates, signs = lane_rates(width, lanes)
        angle = starts * rates[None, :]
        rows += [np.cos(angle), np.sin(angle) * signs[None, :]]
    return jnp.asarray(np.stack(rows).reshape(4, places, length // SPAN, lanes), F32)


def lane_iota(shape):
    return lax.broadcasted_iota(jnp.int32, shape, 1)


def rotary(x, cos_at, sin_at, width):
    half = width // 2
    lanes = x.shape[1]
    if lanes == width:
        other = pltpu.roll(x, half, 1)
    else:
        other = jnp.where(
            lane_iota(x.shape) % width < half,
            pltpu.roll(x, lanes - half, 1),
            pltpu.roll(x, half, 1),
        )
    return x * cos_at + other * sin_at


def full_tables(cos_r, sin_r, rows, at):
    cos_all, sin_all = [], []
    for n in range(rows.shape[1]):
        cos_p, sin_p = rows[at, n : n + 1, :], rows[at + 1, n : n + 1, :]
        cos_all.append(cos_r * cos_p - sin_r * sin_p)
        sin_all.append(sin_r * cos_p + cos_r * sin_p)
    return jnp.concatenate(cos_all, axis=0), jnp.concatenate(sin_all, axis=0)


def by_head(low, high, lanes):
    rows = low.shape[0]
    return jnp.where(lane_iota((rows, lanes)) < HDN, low, high)


def state_kernel(kw, vw, kn, vn, dw, dn, rows, cwr, swr, cnr, snr, out, col, row):
    length, lanes = kw.shape
    head = lax.broadcasted_iota(jnp.int32, (8, length), 0)
    c = jnp.where(head == 0, dw[0:1, :], 0.0)
    for n in range(dn.shape[0]):
        c = jnp.where(head == n + 1, dn[n : n + 1, :], c)
    step = 1
    while step < length:
        c = c + jnp.where(lane_iota(c.shape) >= step, pltpu.roll(c, step, 1), 0.0)
        step *= 2
    row[...] = c
    c = c.T
    col[...] = c
    last = c[length - 1 : length, :]
    tail = jnp.exp(last - c)
    cos_w, sin_w = full_tables(cwr[...], swr[...], rows[...], 0)
    k = rotary(kw[...].astype(F32), cos_w, sin_w, HDW) * (HDW ** (-0.5)) * tail[:, 0:1]
    wide = lax.dot_general(
        k.astype(BF16), vw[...], (((0,), (0,)), ((), ())), preferred_element_type=F32
    )
    cos_n, sin_n = full_tables(cnr[...], snr[...], rows[...], 2)
    k = rotary(kn[...].astype(F32), cos_n, sin_n, HDN) * (HDN ** (-0.5))
    k = k * by_head(tail[:, 1:2], tail[:, 2:3], lanes)
    both = lax.dot_general(
        k.astype(BF16), vn[...], (((0,), (0,)), ((), ())), preferred_element_type=F32
    )
    narrow = jnp.where(lane_iota((HDN, lanes)) < HDN, both[:HDN], both[HDN:])
    total = jnp.exp(last)
    row_w = jnp.broadcast_to(total[:, 0:1], (8, lanes))
    row_n = jnp.broadcast_to(by_head(total[:, 1:2], total[:, 2:3], lanes), (8, lanes))
    out[...] = jnp.concatenate([wide, narrow, row_w, row_n], axis=0).astype(BF16)


def local_kernel(qw, kw, vw, qn, kn, vn, col, row, rows, cwr, swr, cnr, snr, ow, on, qws, qns):
    length, lanes = kw.shape
    size = 256 if length % 256 == 0 else 128
    blocks = length // size
    c = col[...]
    grown = jnp.exp(c)

    def turned(q, k, cos_r, sin_r, at, width):
        cos_at, sin_at = full_tables(cos_r[...], sin_r[...], rows[...], at)
        return (
            rotary(q[...].astype(F32), cos_at, sin_at, width),
            (rotary(k[...].astype(F32), cos_at, sin_at, width) * width ** (-0.5)).astype(BF16),
        )

    def attend(q, k, v, i, head):
        total = None
        for j in range(i + 1):
            scores = lax.dot_general(
                q, k[j * size : (j + 1) * size], (((1,), (1,)), ((), ())), preferred_element_type=F32
            )
            spread = c[i * size : (i + 1) * size, head : head + 1] - row[
                head : head + 1, j * size : (j + 1) * size
            ]
            factor = jnp.exp(jnp.minimum(spread, 0.0))
            if i == j:
                t = lax.broadcasted_iota(jnp.int32, (size, size), 0)
                s = lax.broadcasted_iota(jnp.int32, (size, size), 1)
                factor = jnp.where(t >= s, factor, 0.0)
            part = jnp.dot(
                (scores * factor).astype(BF16),
                v[j * size : (j + 1) * size, :],
                preferred_element_type=F32,
            )
            total = part if total is None else total + part
        return total

    q, k = turned(qw, kw, cwr, swr, 0, HDW)
    qws[...] = (q * grown[:, 0:1]).astype(BF16)
    q = q.astype(BF16)
    for i in range(blocks):
        ow[i * size : (i + 1) * size, :] = attend(q[i * size : (i + 1) * size], k, vw, i, 0)
    q, k = turned(qn, kn, cnr, snr, 2, HDN)
    qns[...] = (q * by_head(grown[:, 1:2], grown[:, 2:3], lanes)).astype(BF16)
    for i in range(blocks):
        part = q[i * size : (i + 1) * size]
        low = lane_iota(part.shape) < HDN
        first = attend(jnp.where(low, part, 0.0).astype(BF16), k, vn, i, 1)
        second = attend(jnp.where(low, 0.0, part).astype(BF16), k, vn, i, 2)
        on[i * size : (i + 1) * size, :] = jnp.where(low, first, second)


STATE = HDW + HDN


def decays(pack):
    lanes = pack.shape[1]
    return jnp.concatenate(
        [
            jnp.broadcast_to(pack[STATE : STATE + 1], (HDW, lanes)),
            jnp.broadcast_to(pack[STATE + 8 : STATE + 9], (HDN, lanes)),
        ],
        axis=0,
    )


def ordered(late, own, other):
    flag = late[0] == 1
    own, other = own[...].astype(F32), other[...].astype(F32)
    return jnp.where(flag, other, own), jnp.where(flag, own, other)


def pair_kernel(late, own, other, out):
    first, second = ordered(late, own, other)
    out[...] = jnp.concatenate(
        [first[:STATE] * decays(second) + second[:STATE], first[STATE:] * second[STATE:]], axis=0
    ).astype(BF16)


def finish_kernel(tp, late, own, other, ow, on, qws, qns, gw, gn, *refs):
    earlier, outs, out = refs[: -tp - 1], refs[-tp - 1 : -1], refs[-1]
    lanes = ow.shape[1]
    state, decay = None, None
    for got in earlier:
        got = got[...].astype(F32)
        state = got[:STATE] if state is None else state + got[:STATE] * decay
        decay = decays(got) if decay is None else decay * decays(got)
    first, _ = ordered(late, own, other)
    state = jnp.where(late[0] == 1, state * decays(first) + first[:STATE], state).astype(BF16)
    wide = ow[...] + jnp.dot(qws[...], state[0:HDW, :], preferred_element_type=F32)
    packed = state[HDW:STATE, :]
    low = lane_iota(packed.shape) < HDN
    zero = jnp.zeros_like(packed)
    square = jnp.concatenate(
        [jnp.where(low, packed, zero), jnp.where(low, zero, packed)], axis=0
    )
    narrow = on[...] + jnp.dot(qns[...], square, preferred_element_type=F32)

    def gated(normed, gate):
        g = gate[...].astype(F32)
        return (g / (1.0 + jnp.exp(-g)) * normed).astype(BF16)

    centre = wide - jnp.mean(wide, axis=1, keepdims=True)
    spread = jnp.mean(centre * centre, axis=1, keepdims=True)
    out[:, 0:lanes] = gated(centre * lax.rsqrt(spread + head_eps), gw)

    low = lane_iota(narrow.shape) < HDN

    def head_mean(x):
        first = jnp.sum(jnp.where(low, x, 0.0), axis=1, keepdims=True)
        second = jnp.sum(jnp.where(low, 0.0, x), axis=1, keepdims=True)
        return jnp.where(low, first, second) * (1.0 / HDN)

    centre = narrow - head_mean(narrow)
    out[:, lanes : 2 * lanes] = gated(
        centre * lax.rsqrt(head_mean(centre * centre) + head_eps), gn
    )
    piece = outs[0].shape[0]
    for m, rows in enumerate(outs):
        start = pl.multiple_of(late[1 + m] * piece, 16)
        rows[...] = out[pl.ds(start, piece), :]


def middle_kernel(stream, gain, wide, narrow, *refs):
    *inputs, middle, normed, turned = refs
    count = (len(inputs) + 1) // 2
    pieces, weights = inputs[:count], inputs[count:]
    half = stream.shape[0] // 2
    total = jnp.dot(
        jnp.concatenate([piece[...] for piece in pieces], axis=1),
        jnp.concatenate([weight[...] for weight in (wide, narrow, *weights)], axis=0),
        preferred_element_type=F32,
    )
    rounded = (stream[...].astype(F32) + total).astype(BF16)
    middle[...] = rounded
    x = rounded.astype(F32)
    scale = lax.rsqrt(jnp.mean(x * x, axis=-1, keepdims=True) + norm_eps)
    result = (x * scale * gain[...].astype(F32)).astype(BF16)
    normed[...] = result
    turned[0:half, :] = result[half:]
    turned[half:, :] = result[:half]


def up_kernel(at, *refs):
    pieces, blocks, (partial, rest, x, ordered_x) = refs[:5], refs[5:-4], refs[-4:]
    depth = blocks[0].shape[0]

    def at_block(n):
        return pl.ds(pl.multiple_of(at[n] * depth, 128), depth)

    @pl.when(pl.program_id(0) == 0)
    def _():
        own, by_x, by_y, low, high = pieces
        rows, half = own.shape[0], low.shape[0]
        x[0:rows, :] = own[...]
        x[rows : 2 * rows, :] = by_x[...]
        x[2 * rows : 2 * rows + half, :] = by_y[half:rows, :]
        x[2 * rows + half : 3 * rows, :] = by_y[0:half, :]
        x[3 * rows : 3 * rows + half, :] = low[...]
        x[3 * rows + half : 4 * rows, :] = high[...]
        for n in range(rest.shape[1] // depth):
            rest[:, n * depth : (n + 1) * depth] = x[:, at_block(len(blocks) + n)]

        for n in range(len(blocks)):
            ordered_x[:, n * depth : (n + 1) * depth] = x[:, at_block(n)]

    weight = jnp.concatenate([block[...] for block in blocks], axis=0)
    partial[...] = jnp.dot(ordered_x[...], weight, preferred_element_type=F32)


def up_most(at, pieces, blocks):
    width = blocks[0].shape[1]
    rows, depth = sum(p.shape[0] for p in pieces), pieces[0].shape[1]
    rest = depth - len(blocks) * blocks[0].shape[0]
    tile = 512
    run = pl.pallas_call(
        up_kernel,
        out_shape=(
            jax.ShapeDtypeStruct((rows, width), F32),
            jax.ShapeDtypeStruct((rows, rest), BF16),
        ),
        grid_spec=pltpu.PrefetchScalarGridSpec(
            num_scalar_prefetch=1,
            grid=(width // tile,),
            in_specs=[pl.BlockSpec(p.shape, lambda n, a: (0, 0)) for p in pieces]
            + [pl.BlockSpec((b.shape[0], tile), lambda n, a: (0, n)) for b in blocks],
            out_specs=(
                pl.BlockSpec((rows, tile), lambda n, a: (0, n)),
                pl.BlockSpec((rows, rest), lambda n, a: (0, 0)),
            ),
            scratch_shapes=[
                pltpu.VMEM((rows, depth), BF16), pltpu.VMEM((rows, depth - rest), BF16)
            ],
        ),
        cost_estimate=pl.CostEstimate(
            flops=2 * rows * (depth - rest) * width,
            bytes_accessed=2 * (rows * depth + depth * width + 2 * rows * width),
            transcendentals=0,
        ),
    )
    return run(at, *pieces, *blocks)


def up_rest(partial, x, blocks):
    total = partial + jnp.dot(
        x, jnp.concatenate(blocks, axis=0), preferred_element_type=F32
    )
    return jnp.square(jax.nn.relu(total)).astype(BF16)


UNIT = 128


def place_kernel(at, middle, *refs):
    *parts, out = refs
    place = 0
    for n in range(0, len(parts), 4):
        group = parts[n : n + 4]
        side = min(group[0].shape[1] // 2, 2 * UNIT)
        for m in range(group[0].shape[1] // side):
            here = slice(m * side, (m + 1) * side)
            columns = pl.ds(pl.multiple_of(at[place] * UNIT, UNIT), side)
            place += 1
            total = middle[:, columns].astype(F32)
            for part in group:
                total = total + part[:, here].astype(F32)
            out[:, columns] = total.astype(BF16)


def pause_kernel(seen, out):
    out[...] = seen[0:8, :].astype(F32)


def hold(seen):
    run = pl.pallas_call(
        pause_kernel,
        out_shape=jax.ShapeDtypeStruct((8, seen.shape[1]), F32),
        in_specs=[VM],
        out_specs=VM,
        compiler_params=pltpu.CompilerParams(has_side_effects=True),
    )
    return run(seen)


def last_kernel(at, out_in, middle, *refs):
    *parts, out = refs
    total = middle[...].astype(F32)
    for part in parts:
        total = total + part[...].astype(F32)
    out[...] = total.astype(BF16)


def place_last(at, out, middle, parts):
    rows = middle.shape[0]
    side = parts[0].shape[1] // 2
    skip = at.shape[0] - 2

    def column(n, a):
        return (0, a[skip + n] // (side // UNIT))

    run = pl.pallas_call(
        last_kernel,
        out_shape=jax.ShapeDtypeStruct(middle.shape, BF16),
        grid_spec=pltpu.PrefetchScalarGridSpec(
            num_scalar_prefetch=1,
            grid=(2,),
            in_specs=[pl.BlockSpec(memory_space=pl.ANY), pl.BlockSpec((rows, side), column)]
            + [pl.BlockSpec((rows, side), lambda n, a: (0, n))] * len(parts),
            out_specs=pl.BlockSpec((rows, side), column),
        ),
        input_output_aliases={1: 0},
        cost_estimate=pl.CostEstimate(
            flops=middle.size, bytes_accessed=4 * middle.size, transcendentals=0
        ),
    )
    return run(at, out, middle, *parts)


def exchange(array, axis, size, move):
    pairs = [(i, move(i)) for i in range(size)]
    return lax.ppermute(array, axis, [(i, j) for i, j in pairs if j is not None and 0 <= j < size])


def retention(tensors, sp, tp):
    (qw, kw, vw, gw, dw, qn, kn, vn, gn, dn) = tensors
    length, lanes = qw.shape
    rows = lax.dynamic_index_in_dim(
        start_rows(sp, length, lanes), lax.axis_index("sp"), 1, keepdims=False
    )
    tables = offset_tables(SPAN, HDW, lanes) + offset_tables(SPAN, HDN, lanes)
    sds = jax.ShapeDtypeStruct
    unit = length * lanes
    state, col, running = call(
        state_kernel,
        (sds((STATE + 16, lanes), BF16), sds((length, 8), F32), sds((8, length), F32)),
        11,
        4 * unit * lanes,
        24 * unit,
    )(kw, vw, kn, vn, dw, dn, rows, *tables)
    ow, on, qws, qns = call(
        local_kernel,
        (sds((length, lanes), F32),) * 2 + (sds((length, lanes), BF16),) * 2,
        13,
        8 * unit * length,
        40 * unit,
    )(qw, kw, vw, qn, kn, vn, col, running, rows, *tables)
    mine = lax.axis_index("tp")
    late = jnp.stack([lax.axis_index("sp") % 2] + [mine ^ m for m in range(tp)]).astype(jnp.int32)
    other = exchange(state, "sp", sp, lambda i: i ^ 1)
    pair = scalar_call(pair_kernel, sds(state.shape, BF16), 2, unit, 6 * state.size)(
        late, state, other
    )
    earlier = [exchange(pair, "sp", sp, lambda i: i + 2 * n) for n in range(1, sp // 2)]
    pieces = scalar_call(
        functools.partial(finish_kernel, tp),
        (sds((length // tp, 2 * lanes), BF16),) * tp,
        8 + len(earlier),
        4 * unit * lanes,
        24 * unit,
        [pltpu.VMEM((length, 2 * lanes), BF16)],
    )(late, state, other, ow, on, qws, qns, gw, gn, *earlier)
    return pieces, other


def to_middle(mixed, stream_in, output_wide, output_narrow, norm_gain, tp):
    weights = [jnp.concatenate([output_wide, output_narrow], axis=0)]
    pieces = [mixed[0]]
    for m in range(1, tp):
        low = m & (m - 1)
        weights.append(exchange(weights[low], "tp", tp, lambda i: i ^ (m ^ low)))
        pieces.append(exchange(mixed[m], "tp", tp, lambda i: i ^ m))
    rows, depth = stream_in.shape
    return call(
        middle_kernel,
        (jax.ShapeDtypeStruct((rows, depth), BF16),) * 3,
        3 + 2 * tp,
        2 * rows * mixed[0].shape[1] * tp * depth,
        8 * stream_in.size,
    )(stream_in, norm_gain[None, :], output_wide, output_narrow, *pieces, *weights[1:])


def tie(array, *after):
    return lax.optimization_barrier((array, *after))[0]


def plane_layer(tensors, stream_in, output_wide, output_narrow, norm_gain, up_weight, down_weight, sp, tp):
    z, y = lax.axis_index("sp") // 2, lax.axis_index("sp") % 2
    core = lax.axis_index("tp") % 2
    at_end = (z == 0) | (z == 3)

    def swap_y_core(array, after=()):
        def move(i):
            s, t = divmod(i, tp)
            return None if s & 1 == t & 1 else (s ^ 1) * tp + (t ^ 1)

        return exchange(tie(array, *after), ("sp", "tp"), sp * tp, move)

    def along_z(array, table):
        def move(i):
            return table[i // 2] * 2 + i % 2 if i // 2 in table else None

        return exchange(array, "sp", sp, move)

    def ends(array):
        return along_z(array, {0: 1, 1: 0, 2: 3, 3: 2})

    def middles(array):
        return along_z(array, {1: 2, 2: 1})

    def outwards(array):
        return along_z(array, {1: 0, 2: 3})

    def by_x(array):
        return exchange(array, "tp", tp, lambda i: i ^ 2)

    def by_y(array):
        return exchange(array, "sp", sp, lambda i: i ^ 1)

    def both_cores(slot):
        return [slot, exchange(slot, "tp", tp, lambda i: i ^ 1)]

    slots = [z, z ^ 1, (z + 2) % 4, (z ^ 1) ^ 2]
    order = jnp.stack([s * 2 + c for s in slots for c in (core, 1 - core)]).astype(jnp.int32)

    def own_block(block, after=()):
        swapped = swap_y_core(block, after)
        return jnp.where(y == core, block, swapped)

    up_own = own_block(up_weight)
    up_near, up_cross = ends(up_own), middles(up_own)

    mixed, other_state = retention(tensors, sp, tp)

    down_own = own_block(down_weight, (other_state,))
    down_near = ends(down_own)
    up_in = middles(up_near)
    up_out = outwards(up_cross)
    down_cross = middles(tie(down_own, up_near))
    up_last = outwards(up_in)

    middle, normed, turned = to_middle(
        mixed, stream_in, output_wide, output_narrow, norm_gain, tp
    )

    half = normed.shape[0] // 2
    x_rows, y_rows = by_x(normed), by_y(turned)
    down_in = middles(down_near)
    d_low, d_high = by_y(x_rows[:half]), by_x(y_rows[:half])

    down_out = outwards(down_cross)
    up_blocks = both_cores(up_own) + both_cores(up_near)
    up_far = jnp.where(at_end, tie(up_out, up_blocks[-1]), up_in)
    up_blocks += both_cores(up_far)
    down_first = both_cores(down_own) + both_cores(down_near)
    partial, rest = up_most(order, [normed, x_rows, y_rows, d_low, d_high], up_blocks)
    up_final = jnp.where(at_end, tie(up_last, partial), up_cross)
    down_last = outwards(tie(down_in, up_final))
    hidden = up_rest(partial, rest, both_cores(up_final))

    parts = {}

    def down(n, blocks):
        part = jnp.dot(
            hidden, jnp.concatenate(blocks, axis=1), preferred_element_type=F32
        ).astype(BF16)
        rows = part.shape[0] // 4
        keep, to_x, to_y, across = (part[m * rows : (m + 1) * rows] for m in range(4))
        parts[n] = part
        return [
            keep,
            exchange(across, ("sp", "tp"), sp * tp, lambda i: i ^ tp ^ 2),
            by_x(to_x),
            by_y(to_y),
        ]

    sums = down(0, down_first)
    down_far = jnp.where(at_end, tie(down_out, parts[0]), down_in)
    sums += down(1, both_cores(down_far))
    pause = hold(stream_in[:16, :128])
    ends_final = both_cores(tie(down_last, parts[1], pause))
    middles_final = both_cores(down_cross)
    sums += down(2, [jnp.where(at_end, a, b) for a, b in zip(ends_final, middles_final)])
    units = 2 * order
    out = scalar_call(
        place_kernel,
        jax.ShapeDtypeStruct(middle.shape, BF16),
        1 + len(sums[:-4]),
        middle.size,
        8 * middle.size,
    )(units, middle, *sums[:-4])
    return place_last(units, out, middle, sums[-4:])


def group_feed_forward(middle, normed):
    def run(up_weight, down_weight):
        rows = lax.all_gather(normed, "tp", axis=0, tiled=True)
        up_sum = jnp.dot(
            rows, lax.all_gather(up_weight, "sp", axis=0, tiled=True), preferred_element_type=F32
        )
        hidden = jnp.square(jax.nn.relu(up_sum)).astype(BF16)
        down_sum = jnp.dot(
            hidden, lax.all_gather(down_weight, "sp", axis=1, tiled=True), preferred_element_type=F32
        )
        down_rows = lax.psum_scatter(
            down_sum.astype(BF16), "tp", scatter_dimension=0, tiled=True
        ).astype(F32)
        return (middle.astype(F32) + down_rows).astype(BF16)

    return run


def on_device(sp, tp, stream_in, *rest):
    *tensors, output_wide, output_narrow, norm_gain, up_weight, down_weight = rest
    if sp == 8 and tp == 4:
        return plane_layer(
            tensors, stream_in, output_wide, output_narrow, norm_gain, up_weight, down_weight, sp, tp
        )
    mixed, _ = retention(tensors, sp, tp)
    middle, normed, _ = to_middle(mixed, stream_in, output_wide, output_narrow, norm_gain, tp)
    return group_feed_forward(middle, normed)(up_weight, down_weight)


def solution(mesh):
    split = P("sp", "tp")
    in_specs = (
        (P(("sp", "tp"), None),)
        + ((split,) * 4 + (P("tp", "sp"),)) * 2
        + (P("tp", None), P("tp", None), P(), split, P("tp", "sp"))
    )
    sp, tp = mesh.shape["sp"], mesh.shape["tp"]
    return jax.shard_map(
        functools.partial(on_device, sp, tp),
        mesh=mesh,
        in_specs=in_specs,
        out_specs=P(("sp", "tp"), None),
        check_vma=False,
    )
```

```python
import functools

import jax
import jax.numpy as jnp
import numpy as np
from jax import lax
from jax.experimental import pallas as pl
from jax.experimental.pallas import tpu as pltpu
from jax.sharding import PartitionSpec as P


HDW = 128
HDN = 64
SPAN = 128

head_eps = 1e-05
norm_eps = 1e-06
rope_base = 10000.0


F32 = jnp.float32
BF16 = jnp.bfloat16
VM = pl.BlockSpec(memory_space=pltpu.VMEM)


def call(kernel, out_shape, count, flops, nbytes):
    return pl.pallas_call(
        kernel,
        out_shape=out_shape,
        in_specs=[VM] * count,
        out_specs=jax.tree.map(lambda _: VM, out_shape),
        cost_estimate=pl.CostEstimate(flops=flops, bytes_accessed=nbytes, transcendentals=0),
    )


def scalar_call(kernel, out_shape, count, flops, nbytes, scratch=()):
    return pl.pallas_call(
        kernel,
        out_shape=out_shape,
        in_specs=[pl.BlockSpec(memory_space=pltpu.SMEM)] + [VM] * count,
        out_specs=jax.tree.map(lambda _: VM, out_shape),
        scratch_shapes=scratch,
        cost_estimate=pl.CostEstimate(flops=flops, bytes_accessed=nbytes, transcendentals=0),
    )


def lane_rates(width, lanes):
    half = width // 2
    lane = np.arange(lanes) % width
    return rope_base ** (-(lane % half).astype(np.float64) / half), np.where(lane < half, -1.0, 1.0)


def offset_tables(length, width, lanes):
    rates, signs = lane_rates(width, lanes)
    angles = np.arange(length, dtype=np.float64)[:, None] * rates[None, :]
    return (
        jnp.asarray(np.cos(angles), F32),
        jnp.asarray(np.sin(angles) * signs[None, :], F32),
    )


def start_rows(places, length, lanes):
    starts = SPAN * np.arange(places * (length // SPAN), dtype=np.float64)[:, None]
    rows = []
    for width in (HDW, HDN):
        rates, signs = lane_rates(width, lanes)
        angle = starts * rates[None, :]
        rows += [np.cos(angle), np.sin(angle) * signs[None, :]]
    return jnp.asarray(np.stack(rows).reshape(4, places, length // SPAN, lanes), F32)


def lane_iota(shape):
    return lax.broadcasted_iota(jnp.int32, shape, 1)


def rotary(x, cos_at, sin_at, width):
    half = width // 2
    lanes = x.shape[1]
    if lanes == width:
        other = pltpu.roll(x, half, 1)
    else:
        other = jnp.where(
            lane_iota(x.shape) % width < half,
            pltpu.roll(x, lanes - half, 1),
            pltpu.roll(x, half, 1),
        )
    return x * cos_at + other * sin_at


def full_tables(cos_r, sin_r, rows, at):
    cos_all, sin_all = [], []
    for n in range(rows.shape[1]):
        cos_p, sin_p = rows[at, n : n + 1, :], rows[at + 1, n : n + 1, :]
        cos_all.append(cos_r * cos_p - sin_r * sin_p)
        sin_all.append(sin_r * cos_p + cos_r * sin_p)
    return jnp.concatenate(cos_all, axis=0), jnp.concatenate(sin_all, axis=0)


def by_head(low, high, lanes):
    rows = low.shape[0]
    return jnp.where(lane_iota((rows, lanes)) < HDN, low, high)


def state_kernel(kw, vw, kn, vn, dw, dn, rows, cwr, swr, cnr, snr, out, col, row):
    length, lanes = kw.shape
    head = lax.broadcasted_iota(jnp.int32, (8, length), 0)
    c = jnp.where(head == 0, dw[0:1, :], 0.0)
    for n in range(dn.shape[0]):
        c = jnp.where(head == n + 1, dn[n : n + 1, :], c)
    step = 1
    while step < length:
        c = c + jnp.where(lane_iota(c.shape) >= step, pltpu.roll(c, step, 1), 0.0)
        step *= 2
    row[...] = c
    c = c.T
    col[...] = c
    last = c[length - 1 : length, :]
    tail = jnp.exp(last - c)
    cos_w, sin_w = full_tables(cwr[...], swr[...], rows[...], 0)
    k = rotary(kw[...].astype(F32), cos_w, sin_w, HDW) * (HDW ** (-0.5)) * tail[:, 0:1]
    wide = lax.dot_general(
        k.astype(BF16), vw[...], (((0,), (0,)), ((), ())), preferred_element_type=F32
    )
    cos_n, sin_n = full_tables(cnr[...], snr[...], rows[...], 2)
    k = rotary(kn[...].astype(F32), cos_n, sin_n, HDN) * (HDN ** (-0.5))
    k = k * by_head(tail[:, 1:2], tail[:, 2:3], lanes)
    both = lax.dot_general(
        k.astype(BF16), vn[...], (((0,), (0,)), ((), ())), preferred_element_type=F32
    )
    narrow = jnp.where(lane_iota((HDN, lanes)) < HDN, both[:HDN], both[HDN:])
    total = jnp.exp(last)
    row_w = jnp.broadcast_to(total[:, 0:1], (8, lanes))
    row_n = jnp.broadcast_to(by_head(total[:, 1:2], total[:, 2:3], lanes), (8, lanes))
    out[...] = jnp.concatenate([wide, narrow, row_w, row_n], axis=0).astype(BF16)


def local_kernel(qw, kw, vw, qn, kn, vn, col, row, rows, cwr, swr, cnr, snr, ow, on, qws, qns):
    length, lanes = kw.shape
    size = 256 if length % 256 == 0 else 128
    blocks = length // size
    c = col[...]
    grown = jnp.exp(c)

    def turned(q, k, cos_r, sin_r, at, width):
        cos_at, sin_at = full_tables(cos_r[...], sin_r[...], rows[...], at)
        return (
            rotary(q[...].astype(F32), cos_at, sin_at, width),
            (rotary(k[...].astype(F32), cos_at, sin_at, width) * width ** (-0.5)).astype(BF16),
        )

    def attend(q, k, v, i, head):
        total = None
        for j in range(i + 1):
            scores = lax.dot_general(
                q, k[j * size : (j + 1) * size], (((1,), (1,)), ((), ())), preferred_element_type=F32
            )
            spread = c[i * size : (i + 1) * size, head : head + 1] - row[
                head : head + 1, j * size : (j + 1) * size
            ]
            factor = jnp.exp(jnp.minimum(spread, 0.0))
            if i == j:
                t = lax.broadcasted_iota(jnp.int32, (size, size), 0)
                s = lax.broadcasted_iota(jnp.int32, (size, size), 1)
                factor = jnp.where(t >= s, factor, 0.0)
            part = jnp.dot(
                (scores * factor).astype(BF16),
                v[j * size : (j + 1) * size, :],
                preferred_element_type=F32,
            )
            total = part if total is None else total + part
        return total

    q, k = turned(qw, kw, cwr, swr, 0, HDW)
    qws[...] = (q * grown[:, 0:1]).astype(BF16)
    q = q.astype(BF16)
    for i in range(blocks):
        ow[i * size : (i + 1) * size, :] = attend(q[i * size : (i + 1) * size], k, vw, i, 0)
    q, k = turned(qn, kn, cnr, snr, 2, HDN)
    qns[...] = (q * by_head(grown[:, 1:2], grown[:, 2:3], lanes)).astype(BF16)
    for i in range(blocks):
        part = q[i * size : (i + 1) * size]
        low = lane_iota(part.shape) < HDN
        first = attend(jnp.where(low, part, 0.0).astype(BF16), k, vn, i, 1)
        second = attend(jnp.where(low, 0.0, part).astype(BF16), k, vn, i, 2)
        on[i * size : (i + 1) * size, :] = jnp.where(low, first, second)


STATE = HDW + HDN


def decays(pack):
    lanes = pack.shape[1]
    return jnp.concatenate(
        [
            jnp.broadcast_to(pack[STATE : STATE + 1], (HDW, lanes)),
            jnp.broadcast_to(pack[STATE + 8 : STATE + 9], (HDN, lanes)),
        ],
        axis=0,
    )


def ordered(late, own, other):
    flag = late[0] == 1
    own, other = own[...].astype(F32), other[...].astype(F32)
    return jnp.where(flag, other, own), jnp.where(flag, own, other)


def pair_kernel(late, own, other, out):
    first, second = ordered(late, own, other)
    out[...] = jnp.concatenate(
        [first[:STATE] * decays(second) + second[:STATE], first[STATE:] * second[STATE:]], axis=0
    ).astype(BF16)


def finish_kernel(tp, late, own, other, ow, on, qws, qns, gw, gn, *refs):
    earlier, outs, out = refs[: -tp - 1], refs[-tp - 1 : -1], refs[-1]
    lanes = ow.shape[1]
    state, decay = None, None
    for got in earlier:
        got = got[...].astype(F32)
        state = got[:STATE] if state is None else state + got[:STATE] * decay
        decay = decays(got) if decay is None else decay * decays(got)
    first, _ = ordered(late, own, other)
    state = jnp.where(late[0] == 1, state * decays(first) + first[:STATE], state).astype(BF16)
    wide = ow[...] + jnp.dot(qws[...], state[0:HDW, :], preferred_element_type=F32)
    packed = state[HDW:STATE, :]
    low = lane_iota(packed.shape) < HDN
    zero = jnp.zeros_like(packed)
    square = jnp.concatenate(
        [jnp.where(low, packed, zero), jnp.where(low, zero, packed)], axis=0
    )
    narrow = on[...] + jnp.dot(qns[...], square, preferred_element_type=F32)

    def gated(normed, gate):
        g = gate[...].astype(F32)
        return (g / (1.0 + jnp.exp(-g)) * normed).astype(BF16)

    centre = wide - jnp.mean(wide, axis=1, keepdims=True)
    spread = jnp.mean(centre * centre, axis=1, keepdims=True)
    out[:, 0:lanes] = gated(centre * lax.rsqrt(spread + head_eps), gw)

    low = lane_iota(narrow.shape) < HDN

    def head_mean(x):
        first = jnp.sum(jnp.where(low, x, 0.0), axis=1, keepdims=True)
        second = jnp.sum(jnp.where(low, 0.0, x), axis=1, keepdims=True)
        return jnp.where(low, first, second) * (1.0 / HDN)

    centre = narrow - head_mean(narrow)
    out[:, lanes : 2 * lanes] = gated(
        centre * lax.rsqrt(head_mean(centre * centre) + head_eps), gn
    )
    piece = outs[0].shape[0]
    for m, rows in enumerate(outs):
        start = pl.multiple_of(late[1 + m] * piece, 16)
        rows[...] = out[pl.ds(start, piece), :]


def middle_kernel(stream, gain, wide, narrow, *refs):
    *inputs, middle, normed, turned = refs
    count = (len(inputs) + 1) // 2
    pieces, weights = inputs[:count], inputs[count:]
    half = stream.shape[0] // 2
    total = jnp.dot(
        jnp.concatenate([piece[...] for piece in pieces], axis=1),
        jnp.concatenate([weight[...] for weight in (wide, narrow, *weights)], axis=0),
        preferred_element_type=F32,
    )
    rounded = (stream[...].astype(F32) + total).astype(BF16)
    middle[...] = rounded
    x = rounded.astype(F32)
    scale = lax.rsqrt(jnp.mean(x * x, axis=-1, keepdims=True) + norm_eps)
    result = (x * scale * gain[...].astype(F32)).astype(BF16)
    normed[...] = result
    turned[0:half, :] = result[half:]
    turned[half:, :] = result[:half]


def up_kernel(at, *refs):
    pieces, blocks, (partial, rest, x, ordered_x) = refs[:5], refs[5:-4], refs[-4:]
    depth = blocks[0].shape[0]

    def at_block(n):
        return pl.ds(pl.multiple_of(at[n] * depth, 128), depth)

    @pl.when(pl.program_id(0) == 0)
    def _():
        own, by_x, by_y, low, high = pieces
        rows, half = own.shape[0], low.shape[0]
        x[0:rows, :] = own[...]
        x[rows : 2 * rows, :] = by_x[...]
        x[2 * rows : 2 * rows + half, :] = by_y[half:rows, :]
        x[2 * rows + half : 3 * rows, :] = by_y[0:half, :]
        x[3 * rows : 3 * rows + half, :] = low[...]
        x[3 * rows + half : 4 * rows, :] = high[...]
        for n in range(rest.shape[1] // depth):
            rest[:, n * depth : (n + 1) * depth] = x[:, at_block(len(blocks) + n)]

        for n in range(len(blocks)):
            ordered_x[:, n * depth : (n + 1) * depth] = x[:, at_block(n)]

    weight = jnp.concatenate([block[...] for block in blocks], axis=0)
    partial[...] = jnp.dot(ordered_x[...], weight, preferred_element_type=F32)


def up_most(at, pieces, blocks):
    width = blocks[0].shape[1]
    rows, depth = sum(p.shape[0] for p in pieces), pieces[0].shape[1]
    rest = depth - len(blocks) * blocks[0].shape[0]
    tile = 512
    run = pl.pallas_call(
        up_kernel,
        out_shape=(
            jax.ShapeDtypeStruct((rows, width), F32),
            jax.ShapeDtypeStruct((rows, rest), BF16),
        ),
        grid_spec=pltpu.PrefetchScalarGridSpec(
            num_scalar_prefetch=1,
            grid=(width // tile,),
            in_specs=[pl.BlockSpec(p.shape, lambda n, a: (0, 0)) for p in pieces]
            + [pl.BlockSpec((b.shape[0], tile), lambda n, a: (0, n)) for b in blocks],
            out_specs=(
                pl.BlockSpec((rows, tile), lambda n, a: (0, n)),
                pl.BlockSpec((rows, rest), lambda n, a: (0, 0)),
            ),
            scratch_shapes=[
                pltpu.VMEM((rows, depth), BF16), pltpu.VMEM((rows, depth - rest), BF16)
            ],
        ),
        cost_estimate=pl.CostEstimate(
            flops=2 * rows * (depth - rest) * width,
            bytes_accessed=2 * (rows * depth + depth * width + 2 * rows * width),
            transcendentals=0,
        ),
    )
    return run(at, *pieces, *blocks)


def up_rest(partial, x, blocks):
    total = partial + jnp.dot(
        x, jnp.concatenate(blocks, axis=0), preferred_element_type=F32
    )
    return jnp.square(jax.nn.relu(total)).astype(BF16)


UNIT = 128


def place_kernel(at, middle, *refs):
    *parts, out = refs
    place = 0
    for n in range(0, len(parts), 4):
        group = parts[n : n + 4]
        side = min(group[0].shape[1] // 2, 2 * UNIT)
        for m in range(group[0].shape[1] // side):
            here = slice(m * side, (m + 1) * side)
            columns = pl.ds(pl.multiple_of(at[place] * UNIT, UNIT), side)
            place += 1
            total = middle[:, columns].astype(F32)
            for part in group:
                total = total + part[:, here].astype(F32)
            out[:, columns] = total.astype(BF16)


def pause_kernel(seen, out):
    out[...] = seen[0:8, :].astype(F32)


def hold(seen):
    run = pl.pallas_call(
        pause_kernel,
        out_shape=jax.ShapeDtypeStruct((8, seen.shape[1]), F32),
        in_specs=[VM],
        out_specs=VM,
        compiler_params=pltpu.CompilerParams(has_side_effects=True),
    )
    return run(seen)


def exchange(array, axis, size, move):
    pairs = [(i, move(i)) for i in range(size)]
    return lax.ppermute(array, axis, [(i, j) for i, j in pairs if j is not None and 0 <= j < size])


def retention(tensors, sp, tp):
    (qw, kw, vw, gw, dw, qn, kn, vn, gn, dn) = tensors
    length, lanes = qw.shape
    rows = lax.dynamic_index_in_dim(
        start_rows(sp, length, lanes), lax.axis_index("sp"), 1, keepdims=False
    )
    tables = offset_tables(SPAN, HDW, lanes) + offset_tables(SPAN, HDN, lanes)
    sds = jax.ShapeDtypeStruct
    unit = length * lanes
    state, col, running = call(
        state_kernel,
        (sds((STATE + 16, lanes), BF16), sds((length, 8), F32), sds((8, length), F32)),
        11,
        4 * unit * lanes,
        24 * unit,
    )(kw, vw, kn, vn, dw, dn, rows, *tables)
    ow, on, qws, qns = call(
        local_kernel,
        (sds((length, lanes), F32),) * 2 + (sds((length, lanes), BF16),) * 2,
        13,
        8 * unit * length,
        40 * unit,
    )(qw, kw, vw, qn, kn, vn, col, running, rows, *tables)
    mine = lax.axis_index("tp")
    late = jnp.stack([lax.axis_index("sp") % 2] + [mine ^ m for m in range(tp)]).astype(jnp.int32)
    other = exchange(state, "sp", sp, lambda i: i ^ 1)
    pair = scalar_call(pair_kernel, sds(state.shape, BF16), 2, unit, 6 * state.size)(
        late, state, other
    )
    earlier = [exchange(pair, "sp", sp, lambda i: i + 2 * n) for n in range(1, sp // 2)]
    pieces = scalar_call(
        functools.partial(finish_kernel, tp),
        (sds((length // tp, 2 * lanes), BF16),) * tp,
        8 + len(earlier),
        4 * unit * lanes,
        24 * unit,
        [pltpu.VMEM((length, 2 * lanes), BF16)],
    )(late, state, other, ow, on, qws, qns, gw, gn, *earlier)
    return pieces, other


def to_middle(mixed, stream_in, output_wide, output_narrow, norm_gain, tp):
    weights = [jnp.concatenate([output_wide, output_narrow], axis=0)]
    pieces = [mixed[0]]
    for m in range(1, tp):
        low = m & (m - 1)
        weights.append(exchange(weights[low], "tp", tp, lambda i: i ^ (m ^ low)))
        pieces.append(exchange(mixed[m], "tp", tp, lambda i: i ^ m))
    rows, depth = stream_in.shape
    return call(
        middle_kernel,
        (jax.ShapeDtypeStruct((rows, depth), BF16),) * 3,
        3 + 2 * tp,
        2 * rows * mixed[0].shape[1] * tp * depth,
        8 * stream_in.size,
    )(stream_in, norm_gain[None, :], output_wide, output_narrow, *pieces, *weights[1:])


def tie(array, *after):
    return lax.optimization_barrier((array, *after))[0]


def plane_layer(tensors, stream_in, output_wide, output_narrow, norm_gain, up_weight, down_weight, sp, tp):
    z, y = lax.axis_index("sp") // 2, lax.axis_index("sp") % 2
    core = lax.axis_index("tp") % 2
    at_end = (z == 0) | (z == 3)

    def swap_y_core(array, after=()):
        def move(i):
            s, t = divmod(i, tp)
            return None if s & 1 == t & 1 else (s ^ 1) * tp + (t ^ 1)

        return exchange(tie(array, *after), ("sp", "tp"), sp * tp, move)

    def along_z(array, table):
        def move(i):
            return table[i // 2] * 2 + i % 2 if i // 2 in table else None

        return exchange(array, "sp", sp, move)

    def ends(array):
        return along_z(array, {0: 1, 1: 0, 2: 3, 3: 2})

    def middles(array):
        return along_z(array, {1: 2, 2: 1})

    def outwards(array):
        return along_z(array, {1: 0, 2: 3})

    def by_x(array):
        return exchange(array, "tp", tp, lambda i: i ^ 2)

    def by_y(array):
        return exchange(array, "sp", sp, lambda i: i ^ 1)

    def both_cores(slot):
        return [slot, exchange(slot, "tp", tp, lambda i: i ^ 1)]

    slots = [z, z ^ 1, (z + 2) % 4, (z ^ 1) ^ 2]
    order = jnp.stack([s * 2 + c for s in slots for c in (core, 1 - core)]).astype(jnp.int32)

    def own_block(block, after=()):
        swapped = swap_y_core(block, after)
        return jnp.where(y == core, block, swapped)

    up_own = own_block(up_weight)
    up_near, up_cross = ends(up_own), middles(up_own)

    mixed, other_state = retention(tensors, sp, tp)

    down_own = own_block(down_weight, (other_state,))
    down_near = ends(down_own)
    up_in = middles(up_near)
    up_out = outwards(up_cross)
    down_cross = middles(tie(down_own, up_near))
    up_last = outwards(up_in)

    middle, normed, turned = to_middle(
        mixed, stream_in, output_wide, output_narrow, norm_gain, tp
    )

    half = normed.shape[0] // 2
    x_rows, y_rows = by_x(normed), by_y(turned)
    down_in = middles(down_near)
    d_low, d_high = by_y(x_rows[:half]), by_x(y_rows[:half])

    down_out = outwards(down_cross)
    up_blocks = both_cores(up_own) + both_cores(up_near)
    up_far = jnp.where(at_end, tie(up_out, up_blocks[-1]), up_in)
    up_blocks += both_cores(up_far)
    down_first = both_cores(down_own) + both_cores(down_near)
    partial, rest = up_most(order, [normed, x_rows, y_rows, d_low, d_high], up_blocks)
    up_final = jnp.where(at_end, tie(up_last, partial), up_cross)
    down_last = outwards(tie(down_in, up_final))
    hidden = up_rest(partial, rest, both_cores(up_final))

    parts = {}

    def down(n, blocks):
        part = jnp.dot(
            hidden, jnp.concatenate(blocks, axis=1), preferred_element_type=F32
        ).astype(BF16)
        rows = part.shape[0] // 4
        keep, to_x, to_y, across = (part[m * rows : (m + 1) * rows] for m in range(4))
        parts[n] = part
        return [
            keep,
            exchange(across, ("sp", "tp"), sp * tp, lambda i: i ^ tp ^ 2),
            by_x(to_x),
            by_y(to_y),
        ]

    sums = down(0, down_first)
    wait = hold(stream_in[32:48, :128])
    down_far = jnp.where(at_end, tie(down_out, parts[0], wait), down_in)
    sums += down(1, both_cores(down_far))
    pause = hold(stream_in[:16, :128])
    ends_final = both_cores(tie(down_last, parts[1], pause))
    middles_final = both_cores(down_cross)
    sums += down(2, [jnp.where(at_end, a, b) for a, b in zip(ends_final, middles_final)])
    units = 2 * order
    out = scalar_call(
        place_kernel,
        jax.ShapeDtypeStruct(middle.shape, BF16),
        1 + len(sums[:-4]),
        middle.size,
        8 * middle.size,
    )(units, middle, *sums[:-4])
    part = sum(p.astype(F32) for p in sums[-4:])
    width = part.shape[1]
    part = jnp.where(core == 0, part, jnp.roll(part, width // 2, axis=1))
    start = slots[3] * width
    part = part + lax.dynamic_slice_in_dim(middle, start, width, 1).astype(F32)
    return lax.dynamic_update_slice_in_dim(out, part.astype(BF16), start, 1)


def group_feed_forward(middle, normed):
    def run(up_weight, down_weight):
        rows = lax.all_gather(normed, "tp", axis=0, tiled=True)
        up_sum = jnp.dot(
            rows, lax.all_gather(up_weight, "sp", axis=0, tiled=True), preferred_element_type=F32
        )
        hidden = jnp.square(jax.nn.relu(up_sum)).astype(BF16)
        down_sum = jnp.dot(
            hidden, lax.all_gather(down_weight, "sp", axis=1, tiled=True), preferred_element_type=F32
        )
        down_rows = lax.psum_scatter(
            down_sum.astype(BF16), "tp", scatter_dimension=0, tiled=True
        ).astype(F32)
        return (middle.astype(F32) + down_rows).astype(BF16)

    return run


def on_device(sp, tp, stream_in, *rest):
    *tensors, output_wide, output_narrow, norm_gain, up_weight, down_weight = rest
    if sp == 8 and tp == 4:
        return plane_layer(
            tensors, stream_in, output_wide, output_narrow, norm_gain, up_weight, down_weight, sp, tp
        )
    mixed, _ = retention(tensors, sp, tp)
    middle, normed, _ = to_middle(mixed, stream_in, output_wide, output_narrow, norm_gain, tp)
    return group_feed_forward(middle, normed)(up_weight, down_weight)


def solution(mesh):
    split = P("sp", "tp")
    in_specs = (
        (P(("sp", "tp"), None),)
        + ((split,) * 4 + (P("tp", "sp"),)) * 2
        + (P("tp", None), P("tp", None), P(), split, P("tp", "sp"))
    )
    sp, tp = mesh.shape["sp"], mesh.shape["tp"]
    return jax.shard_map(
        functools.partial(on_device, sp, tp),
        mesh=mesh,
        in_specs=in_specs,
        out_specs=P(("sp", "tp"), None),
        check_vma=False,
    )
```

```python
import functools

import jax
import jax.numpy as jnp
import numpy as np
from jax import lax
from jax.experimental import pallas as pl
from jax.experimental.pallas import tpu as pltpu
from jax.sharding import PartitionSpec as P


HDW = 128
HDN = 64
SPAN = 128

head_eps = 1e-05
norm_eps = 1e-06
rope_base = 10000.0


F32 = jnp.float32
BF16 = jnp.bfloat16
VM = pl.BlockSpec(memory_space=pltpu.VMEM)


def call(kernel, out_shape, count, flops, nbytes):
    return pl.pallas_call(
        kernel,
        out_shape=out_shape,
        in_specs=[VM] * count,
        out_specs=jax.tree.map(lambda _: VM, out_shape),
        cost_estimate=pl.CostEstimate(flops=flops, bytes_accessed=nbytes, transcendentals=0),
    )


def scalar_call(kernel, out_shape, count, flops, nbytes, scratch=()):
    return pl.pallas_call(
        kernel,
        out_shape=out_shape,
        in_specs=[pl.BlockSpec(memory_space=pltpu.SMEM)] + [VM] * count,
        out_specs=jax.tree.map(lambda _: VM, out_shape),
        scratch_shapes=scratch,
        cost_estimate=pl.CostEstimate(flops=flops, bytes_accessed=nbytes, transcendentals=0),
    )


def lane_rates(width, lanes):
    half = width // 2
    lane = np.arange(lanes) % width
    return rope_base ** (-(lane % half).astype(np.float64) / half), np.where(lane < half, -1.0, 1.0)


def offset_tables(length, width, lanes):
    rates, signs = lane_rates(width, lanes)
    angles = np.arange(length, dtype=np.float64)[:, None] * rates[None, :]
    return (
        jnp.asarray(np.cos(angles), F32),
        jnp.asarray(np.sin(angles) * signs[None, :], F32),
    )


def start_rows(places, length, lanes):
    starts = SPAN * np.arange(places * (length // SPAN), dtype=np.float64)[:, None]
    rows = []
    for width in (HDW, HDN):
        rates, signs = lane_rates(width, lanes)
        angle = starts * rates[None, :]
        rows += [np.cos(angle), np.sin(angle) * signs[None, :]]
    return jnp.asarray(np.stack(rows).reshape(4, places, length // SPAN, lanes), F32)


def lane_iota(shape):
    return lax.broadcasted_iota(jnp.int32, shape, 1)


def rotary(x, cos_at, sin_at, width):
    half = width // 2
    lanes = x.shape[1]
    if lanes == width:
        other = pltpu.roll(x, half, 1)
    else:
        other = jnp.where(
            lane_iota(x.shape) % width < half,
            pltpu.roll(x, lanes - half, 1),
            pltpu.roll(x, half, 1),
        )
    return x * cos_at + other * sin_at


def full_tables(cos_r, sin_r, rows, at):
    cos_all, sin_all = [], []
    for n in range(rows.shape[1]):
        cos_p, sin_p = rows[at, n : n + 1, :], rows[at + 1, n : n + 1, :]
        cos_all.append(cos_r * cos_p - sin_r * sin_p)
        sin_all.append(sin_r * cos_p + cos_r * sin_p)
    return jnp.concatenate(cos_all, axis=0), jnp.concatenate(sin_all, axis=0)


def by_head(low, high, lanes):
    rows = low.shape[0]
    return jnp.where(lane_iota((rows, lanes)) < HDN, low, high)


def state_kernel(kw, vw, kn, vn, dw, dn, rows, cwr, swr, cnr, snr, out, col, row):
    length, lanes = kw.shape
    head = lax.broadcasted_iota(jnp.int32, (8, length), 0)
    c = jnp.where(head == 0, dw[0:1, :], 0.0)
    for n in range(dn.shape[0]):
        c = jnp.where(head == n + 1, dn[n : n + 1, :], c)
    step = 1
    while step < length:
        c = c + jnp.where(lane_iota(c.shape) >= step, pltpu.roll(c, step, 1), 0.0)
        step *= 2
    row[...] = c
    c = c.T
    col[...] = c
    last = c[length - 1 : length, :]
    tail = jnp.exp(last - c)
    cos_w, sin_w = full_tables(cwr[...], swr[...], rows[...], 0)
    k = rotary(kw[...].astype(F32), cos_w, sin_w, HDW) * (HDW ** (-0.5)) * tail[:, 0:1]
    wide = lax.dot_general(
        k.astype(BF16), vw[...], (((0,), (0,)), ((), ())), preferred_element_type=F32
    )
    cos_n, sin_n = full_tables(cnr[...], snr[...], rows[...], 2)
    k = rotary(kn[...].astype(F32), cos_n, sin_n, HDN) * (HDN ** (-0.5))
    k = k * by_head(tail[:, 1:2], tail[:, 2:3], lanes)
    both = lax.dot_general(
        k.astype(BF16), vn[...], (((0,), (0,)), ((), ())), preferred_element_type=F32
    )
    narrow = jnp.where(lane_iota((HDN, lanes)) < HDN, both[:HDN], both[HDN:])
    total = jnp.exp(last)
    row_w = jnp.broadcast_to(total[:, 0:1], (8, lanes))
    row_n = jnp.broadcast_to(by_head(total[:, 1:2], total[:, 2:3], lanes), (8, lanes))
    out[...] = jnp.concatenate([wide, narrow, row_w, row_n], axis=0).astype(BF16)


def local_kernel(qw, kw, vw, qn, kn, vn, col, row, rows, cwr, swr, cnr, snr, ow, on, qws, qns):
    length, lanes = kw.shape
    size = 256 if length % 256 == 0 else 128
    blocks = length // size
    c = col[...]
    grown = jnp.exp(c)

    def turned(q, k, cos_r, sin_r, at, width):
        cos_at, sin_at = full_tables(cos_r[...], sin_r[...], rows[...], at)
        return (
            rotary(q[...].astype(F32), cos_at, sin_at, width),
            (rotary(k[...].astype(F32), cos_at, sin_at, width) * width ** (-0.5)).astype(BF16),
        )

    def attend(q, k, v, i, head):
        total = None
        for j in range(i + 1):
            scores = lax.dot_general(
                q, k[j * size : (j + 1) * size], (((1,), (1,)), ((), ())), preferred_element_type=F32
            )
            spread = c[i * size : (i + 1) * size, head : head + 1] - row[
                head : head + 1, j * size : (j + 1) * size
            ]
            factor = jnp.exp(jnp.minimum(spread, 0.0))
            if i == j:
                t = lax.broadcasted_iota(jnp.int32, (size, size), 0)
                s = lax.broadcasted_iota(jnp.int32, (size, size), 1)
                factor = jnp.where(t >= s, factor, 0.0)
            part = jnp.dot(
                (scores * factor).astype(BF16),
                v[j * size : (j + 1) * size, :],
                preferred_element_type=F32,
            )
            total = part if total is None else total + part
        return total

    q, k = turned(qw, kw, cwr, swr, 0, HDW)
    qws[...] = (q * grown[:, 0:1]).astype(BF16)
    q = q.astype(BF16)
    for i in range(blocks):
        ow[i * size : (i + 1) * size, :] = attend(q[i * size : (i + 1) * size], k, vw, i, 0)
    q, k = turned(qn, kn, cnr, snr, 2, HDN)
    qns[...] = (q * by_head(grown[:, 1:2], grown[:, 2:3], lanes)).astype(BF16)
    for i in range(blocks):
        part = q[i * size : (i + 1) * size]
        low = lane_iota(part.shape) < HDN
        first = attend(jnp.where(low, part, 0.0).astype(BF16), k, vn, i, 1)
        second = attend(jnp.where(low, 0.0, part).astype(BF16), k, vn, i, 2)
        on[i * size : (i + 1) * size, :] = jnp.where(low, first, second)


STATE = HDW + HDN


def decays(pack):
    lanes = pack.shape[1]
    return jnp.concatenate(
        [
            jnp.broadcast_to(pack[STATE : STATE + 1], (HDW, lanes)),
            jnp.broadcast_to(pack[STATE + 8 : STATE + 9], (HDN, lanes)),
        ],
        axis=0,
    )


def ordered(late, own, other):
    flag = late[0] == 1
    own, other = own[...].astype(F32), other[...].astype(F32)
    return jnp.where(flag, other, own), jnp.where(flag, own, other)


def pair_kernel(late, own, other, out):
    first, second = ordered(late, own, other)
    out[...] = jnp.concatenate(
        [first[:STATE] * decays(second) + second[:STATE], first[STATE:] * second[STATE:]], axis=0
    ).astype(BF16)


def finish_kernel(tp, late, own, other, ow, on, qws, qns, gw, gn, *refs):
    earlier, outs, out = refs[: -tp - 1], refs[-tp - 1 : -1], refs[-1]
    lanes = ow.shape[1]
    state, decay = None, None
    for got in earlier:
        got = got[...].astype(F32)
        state = got[:STATE] if state is None else state + got[:STATE] * decay
        decay = decays(got) if decay is None else decay * decays(got)
    first, _ = ordered(late, own, other)
    state = jnp.where(late[0] == 1, state * decays(first) + first[:STATE], state).astype(BF16)
    wide = ow[...] + jnp.dot(qws[...], state[0:HDW, :], preferred_element_type=F32)
    packed = state[HDW:STATE, :]
    low = lane_iota(packed.shape) < HDN
    zero = jnp.zeros_like(packed)
    square = jnp.concatenate(
        [jnp.where(low, packed, zero), jnp.where(low, zero, packed)], axis=0
    )
    narrow = on[...] + jnp.dot(qns[...], square, preferred_element_type=F32)

    def gated(normed, gate):
        g = gate[...].astype(F32)
        return (g / (1.0 + jnp.exp(-g)) * normed).astype(BF16)

    centre = wide - jnp.mean(wide, axis=1, keepdims=True)
    spread = jnp.mean(centre * centre, axis=1, keepdims=True)
    out[:, 0:lanes] = gated(centre * lax.rsqrt(spread + head_eps), gw)

    low = lane_iota(narrow.shape) < HDN

    def head_mean(x):
        first = jnp.sum(jnp.where(low, x, 0.0), axis=1, keepdims=True)
        second = jnp.sum(jnp.where(low, 0.0, x), axis=1, keepdims=True)
        return jnp.where(low, first, second) * (1.0 / HDN)

    centre = narrow - head_mean(narrow)
    out[:, lanes : 2 * lanes] = gated(
        centre * lax.rsqrt(head_mean(centre * centre) + head_eps), gn
    )
    piece = outs[0].shape[0]
    for m, rows in enumerate(outs):
        start = pl.multiple_of(late[1 + m] * piece, 16)
        rows[...] = out[pl.ds(start, piece), :]


def middle_kernel(stream, gain, wide, narrow, *refs):
    *inputs, middle, normed, turned = refs
    count = (len(inputs) + 1) // 2
    pieces, weights = inputs[:count], inputs[count:]
    half = stream.shape[0] // 2
    total = jnp.dot(
        jnp.concatenate([piece[...] for piece in pieces], axis=1),
        jnp.concatenate([weight[...] for weight in (wide, narrow, *weights)], axis=0),
        preferred_element_type=F32,
    )
    rounded = (stream[...].astype(F32) + total).astype(BF16)
    middle[...] = rounded
    x = rounded.astype(F32)
    scale = lax.rsqrt(jnp.mean(x * x, axis=-1, keepdims=True) + norm_eps)
    result = (x * scale * gain[...].astype(F32)).astype(BF16)
    normed[...] = result
    turned[0:half, :] = result[half:]
    turned[half:, :] = result[:half]


def up_kernel(at, *refs):
    pieces, blocks, (partial, rest, x, ordered_x) = refs[:5], refs[5:-4], refs[-4:]
    depth = blocks[0].shape[0]

    def at_block(n):
        return pl.ds(pl.multiple_of(at[n] * depth, 128), depth)

    @pl.when(pl.program_id(0) == 0)
    def _():
        own, by_x, by_y, low, high = pieces
        rows, half = own.shape[0], low.shape[0]
        x[0:rows, :] = own[...]
        x[rows : 2 * rows, :] = by_x[...]
        x[2 * rows : 2 * rows + half, :] = by_y[half:rows, :]
        x[2 * rows + half : 3 * rows, :] = by_y[0:half, :]
        x[3 * rows : 3 * rows + half, :] = low[...]
        x[3 * rows + half : 4 * rows, :] = high[...]
        for n in range(rest.shape[1] // depth):
            rest[:, n * depth : (n + 1) * depth] = x[:, at_block(len(blocks) + n)]

        for n in range(len(blocks)):
            ordered_x[:, n * depth : (n + 1) * depth] = x[:, at_block(n)]

    weight = jnp.concatenate([block[...] for block in blocks], axis=0)
    partial[...] = jnp.dot(ordered_x[...], weight, preferred_element_type=F32)


def up_most(at, pieces, blocks):
    width = blocks[0].shape[1]
    rows, depth = sum(p.shape[0] for p in pieces), pieces[0].shape[1]
    rest = depth - len(blocks) * blocks[0].shape[0]
    tile = 512
    run = pl.pallas_call(
        up_kernel,
        out_shape=(
            jax.ShapeDtypeStruct((rows, width), F32),
            jax.ShapeDtypeStruct((rows, rest), BF16),
        ),
        grid_spec=pltpu.PrefetchScalarGridSpec(
            num_scalar_prefetch=1,
            grid=(width // tile,),
            in_specs=[pl.BlockSpec(p.shape, lambda n, a: (0, 0)) for p in pieces]
            + [pl.BlockSpec((b.shape[0], tile), lambda n, a: (0, n)) for b in blocks],
            out_specs=(
                pl.BlockSpec((rows, tile), lambda n, a: (0, n)),
                pl.BlockSpec((rows, rest), lambda n, a: (0, 0)),
            ),
            scratch_shapes=[
                pltpu.VMEM((rows, depth), BF16), pltpu.VMEM((rows, depth - rest), BF16)
            ],
        ),
        cost_estimate=pl.CostEstimate(
            flops=2 * rows * (depth - rest) * width,
            bytes_accessed=2 * (rows * depth + depth * width + 2 * rows * width),
            transcendentals=0,
        ),
    )
    return run(at, *pieces, *blocks)


def up_rest(partial, x, blocks):
    total = partial + jnp.dot(
        x, jnp.concatenate(blocks, axis=0), preferred_element_type=F32
    )
    return jnp.square(jax.nn.relu(total)).astype(BF16)


UNIT = 128


def place_kernel(at, middle, *refs):
    *parts, out = refs
    place = 0
    for n in range(0, len(parts), 4):
        group = parts[n : n + 4]
        side = min(group[0].shape[1] // 2, 2 * UNIT)
        for m in range(group[0].shape[1] // side):
            here = slice(m * side, (m + 1) * side)
            columns = pl.ds(pl.multiple_of(at[place] * UNIT, UNIT), side)
            place += 1
            total = middle[:, columns].astype(F32)
            for part in group:
                total = total + part[:, here].astype(F32)
            out[:, columns] = total.astype(BF16)


def pause_kernel(seen, out):
    out[...] = seen[0:8, :].astype(F32)


def hold(seen):
    run = pl.pallas_call(
        pause_kernel,
        out_shape=jax.ShapeDtypeStruct((8, seen.shape[1]), F32),
        in_specs=[VM],
        out_specs=VM,
        compiler_params=pltpu.CompilerParams(has_side_effects=True),
    )
    return run(seen)


def exchange(array, axis, size, move):
    pairs = [(i, move(i)) for i in range(size)]
    return lax.ppermute(array, axis, [(i, j) for i, j in pairs if j is not None and 0 <= j < size])


def retention(tensors, sp, tp):
    (qw, kw, vw, gw, dw, qn, kn, vn, gn, dn) = tensors
    length, lanes = qw.shape
    rows = lax.dynamic_index_in_dim(
        start_rows(sp, length, lanes), lax.axis_index("sp"), 1, keepdims=False
    )
    tables = offset_tables(SPAN, HDW, lanes) + offset_tables(SPAN, HDN, lanes)
    sds = jax.ShapeDtypeStruct
    unit = length * lanes
    state, col, running = call(
        state_kernel,
        (sds((STATE + 16, lanes), BF16), sds((length, 8), F32), sds((8, length), F32)),
        11,
        4 * unit * lanes,
        24 * unit,
    )(kw, vw, kn, vn, dw, dn, rows, *tables)
    ow, on, qws, qns = call(
        local_kernel,
        (sds((length, lanes), F32),) * 2 + (sds((length, lanes), BF16),) * 2,
        13,
        8 * unit * length,
        40 * unit,
    )(qw, kw, vw, qn, kn, vn, col, running, rows, *tables)
    mine = lax.axis_index("tp")
    late = jnp.stack([lax.axis_index("sp") % 2] + [mine ^ m for m in range(tp)]).astype(jnp.int32)
    other = exchange(state, "sp", sp, lambda i: i ^ 1)
    pair = scalar_call(pair_kernel, sds(state.shape, BF16), 2, unit, 6 * state.size)(
        late, state, other
    )
    earlier = [exchange(pair, "sp", sp, lambda i: i + 2 * n) for n in range(1, sp // 2)]
    pieces = scalar_call(
        functools.partial(finish_kernel, tp),
        (sds((length // tp, 2 * lanes), BF16),) * tp,
        8 + len(earlier),
        4 * unit * lanes,
        24 * unit,
        [pltpu.VMEM((length, 2 * lanes), BF16)],
    )(late, state, other, ow, on, qws, qns, gw, gn, *earlier)
    return pieces, other


def to_middle(mixed, stream_in, output_wide, output_narrow, norm_gain, tp):
    weights = [jnp.concatenate([output_wide, output_narrow], axis=0)]
    pieces = [mixed[0]]
    for m in range(1, tp):
        low = m & (m - 1)
        weights.append(exchange(weights[low], "tp", tp, lambda i: i ^ (m ^ low)))
        pieces.append(exchange(mixed[m], "tp", tp, lambda i: i ^ m))
    rows, depth = stream_in.shape
    return call(
        middle_kernel,
        (jax.ShapeDtypeStruct((rows, depth), BF16),) * 3,
        3 + 2 * tp,
        2 * rows * mixed[0].shape[1] * tp * depth,
        8 * stream_in.size,
    )(stream_in, norm_gain[None, :], output_wide, output_narrow, *pieces, *weights[1:])


def tie(array, *after):
    return lax.optimization_barrier((array, *after))[0]


def plane_layer(tensors, stream_in, output_wide, output_narrow, norm_gain, up_weight, down_weight, sp, tp):
    z, y = lax.axis_index("sp") // 2, lax.axis_index("sp") % 2
    core = lax.axis_index("tp") % 2
    at_end = (z == 0) | (z == 3)

    def swap_y_core(array, after=()):
        def move(i):
            s, t = divmod(i, tp)
            return None if s & 1 == t & 1 else (s ^ 1) * tp + (t ^ 1)

        return exchange(tie(array, *after), ("sp", "tp"), sp * tp, move)

    def along_z(array, table):
        def move(i):
            return table[i // 2] * 2 + i % 2 if i // 2 in table else None

        return exchange(array, "sp", sp, move)

    def ends(array):
        return along_z(array, {0: 1, 1: 0, 2: 3, 3: 2})

    def middles(array):
        return along_z(array, {1: 2, 2: 1})

    def outwards(array):
        return along_z(array, {1: 0, 2: 3})

    def by_x(array):
        return exchange(array, "tp", tp, lambda i: i ^ 2)

    def by_y(array):
        return exchange(array, "sp", sp, lambda i: i ^ 1)

    def both_cores(slot, planes=range(4)):
        def move(i):
            return i ^ 1 if i // tp // 2 in planes else None

        return [slot, exchange(slot, ("sp", "tp"), sp * tp, move)]

    slots = [z, z ^ 1, (z + 2) % 4, (z ^ 1) ^ 2]
    order = jnp.stack([s * 2 + c for s in slots for c in (core, 1 - core)]).astype(jnp.int32)

    def own_block(block, after=()):
        swapped = swap_y_core(block, after)
        return jnp.where(y == core, block, swapped)

    up_own = own_block(up_weight)
    up_near, up_cross = ends(up_own), middles(up_own)

    mixed, other_state = retention(tensors, sp, tp)

    down_own = own_block(down_weight, (other_state,))
    down_near = ends(down_own)
    up_in = middles(up_near)
    up_out = outwards(up_cross)
    down_cross = middles(tie(down_own, up_near))
    up_last = outwards(up_in)

    middle, normed, turned = to_middle(
        mixed, stream_in, output_wide, output_narrow, norm_gain, tp
    )

    half = normed.shape[0] // 2
    x_rows, y_rows = by_x(normed), by_y(turned)
    down_in = middles(down_near)
    d_low, d_high = by_y(x_rows[:half]), by_x(y_rows[:half])

    down_out = outwards(down_cross)
    up_blocks = both_cores(up_own) + both_cores(up_near)
    up_far = jnp.where(at_end, tie(up_out, up_blocks[-1]), up_in)
    up_blocks += both_cores(up_far)
    down_first = both_cores(down_own) + both_cores(down_near)
    partial, rest = up_most(order, [normed, x_rows, y_rows, d_low, d_high], up_blocks)
    up_final = jnp.where(at_end, tie(up_last, partial), up_cross)
    down_last = outwards(tie(down_in, up_final))
    hidden = up_rest(partial, rest, both_cores(up_final))

    parts = {}

    def down(n, blocks):
        part = jnp.dot(
            hidden, jnp.concatenate(blocks, axis=1), preferred_element_type=F32
        ).astype(BF16)
        rows = part.shape[0] // 4
        keep, to_x, to_y, across = (part[m * rows : (m + 1) * rows] for m in range(4))
        parts[n] = part
        return [
            keep,
            exchange(across, ("sp", "tp"), sp * tp, lambda i: i ^ tp ^ 2),
            by_x(to_x),
            by_y(to_y),
        ]

    sums = down(0, down_first)
    wait = hold(stream_in[32:48, :128])
    down_far = jnp.where(at_end, tie(down_out, parts[0], wait), down_in)
    sums += down(1, both_cores(down_far))
    pause = hold(stream_in[:16, :128])
    ends_final = both_cores(tie(down_last, parts[1], pause), (0, 3))
    middles_final = both_cores(down_cross, (1, 2))
    sums += down(2, [jnp.where(at_end, a, b) for a, b in zip(ends_final, middles_final)])
    units = 2 * order
    out = scalar_call(
        place_kernel,
        jax.ShapeDtypeStruct(middle.shape, BF16),
        1 + len(sums[:-4]),
        middle.size,
        8 * middle.size,
    )(units, middle, *sums[:-4])
    part = sum(p.astype(F32) for p in sums[-4:])
    width = part.shape[1]
    part = jnp.where(core == 0, part, jnp.roll(part, width // 2, axis=1))
    start = slots[3] * width
    part = part + lax.dynamic_slice_in_dim(middle, start, width, 1).astype(F32)
    return lax.dynamic_update_slice_in_dim(out, part.astype(BF16), start, 1)


def group_feed_forward(middle, normed):
    def run(up_weight, down_weight):
        rows = lax.all_gather(normed, "tp", axis=0, tiled=True)
        up_sum = jnp.dot(
            rows, lax.all_gather(up_weight, "sp", axis=0, tiled=True), preferred_element_type=F32
        )
        hidden = jnp.square(jax.nn.relu(up_sum)).astype(BF16)
        down_sum = jnp.dot(
            hidden, lax.all_gather(down_weight, "sp", axis=1, tiled=True), preferred_element_type=F32
        )
        down_rows = lax.psum_scatter(
            down_sum.astype(BF16), "tp", scatter_dimension=0, tiled=True
        ).astype(F32)
        return (middle.astype(F32) + down_rows).astype(BF16)

    return run


def on_device(sp, tp, stream_in, *rest):
    *tensors, output_wide, output_narrow, norm_gain, up_weight, down_weight = rest
    if sp == 8 and tp == 4:
        return plane_layer(
            tensors, stream_in, output_wide, output_narrow, norm_gain, up_weight, down_weight, sp, tp
        )
    mixed, _ = retention(tensors, sp, tp)
    middle, normed, _ = to_middle(mixed, stream_in, output_wide, output_narrow, norm_gain, tp)
    return group_feed_forward(middle, normed)(up_weight, down_weight)


def solution(mesh):
    split = P("sp", "tp")
    in_specs = (
        (P(("sp", "tp"), None),)
        + ((split,) * 4 + (P("tp", "sp"),)) * 2
        + (P("tp", None), P("tp", None), P(), split, P("tp", "sp"))
    )
    sp, tp = mesh.shape["sp"], mesh.shape["tp"]
    return jax.shard_map(
        functools.partial(on_device, sp, tp),
        mesh=mesh,
        in_specs=in_specs,
        out_specs=P(("sp", "tp"), None),
        check_vma=False,
    )
```
